256 devices in a mesh: sp: 32 (over z, x), tp: 8 (over y, core).
Axes of the slice: x: 4, y: 4, z: 8, core: 2. Of those that a mesh axis runs over, the one named last changes fastest.
Arguments:
- out_grad: bfloat16 [4096, 2048], P('sp', 'tp'), may hold values from -6 to 6
- moe_input: bfloat16 [4096, 2048], P('sp', 'tp'), may hold values from -6 to 6
- route_weight: float32 [4096, 2], P('sp'), may hold values from 0.2 to 1
- route_ids: int32 [4096, 2], P('sp'), may hold values from 0 to 31, all different within a row; in each aligned block of 128 rows (0 to 127, 128 to 255, ...) at most 16 rows name the same one
- gate_proj: bfloat16 [32, 2048, 2816], P('sp', None, 'tp'), may hold values from -0.125 to 0.125
- up_proj: bfloat16 [32, 2048, 2816], P('sp', None, 'tp'), may hold values from -0.125 to 0.125
- down_proj: bfloat16 [32, 2816, 2048], P('sp', 'tp'), may hold values from -0.109375 to 0.109375
- out_proj: bfloat16 [2048, 2048], P(None, 'tp'), may hold values from -0.125 to 0.125
- conv_out: bfloat16 [4096, 2048], P('sp', 'tp'), may hold values from -6 to 6
- gate_b: bfloat16 [4096, 2048], P('sp', 'tp'), may hold values from -6 to 6
- gate_c: bfloat16 [4096, 2048], P('sp', 'tp'), may hold values from -6 to 6
- value_v: bfloat16 [4096, 2048], P('sp', 'tp'), may hold values from -6 to 6
- conv_taps: float32 [3, 2048], P(None, 'tp'), may hold values from -3 to 3
Outputs:
- grad_gate: bfloat16 [32, 2048, 2816], P('sp', None, 'tp')
- grad_up: bfloat16 [32, 2048, 2816], P('sp', None, 'tp')
- grad_down: bfloat16 [32, 2816, 2048], P('sp', 'tp')
- grad_out: float32 [2048, 2048], P('sp', 'tp')
- grad_b: bfloat16 [4096, 2048], P('sp', 'tp')
- grad_c: bfloat16 [4096, 2048], P('sp', 'tp')
- grad_v: bfloat16 [4096, 2048], P('sp', 'tp')
The draws below stay inside these ranges and needn't reach their ends.
Inputs may be any that keep to these rules, and one draw needn't show every extreme that they name: `route_ids`: each row names two different experts; within the 128 rows of one index of sp no expert is named by more than 16 rows, a bound that some block reaches.
All inputs are finite; a program needn't handle non-finite values.
Results may differ from the reference program's by a relative error of at most 0.019.
Values may be sent and summed in bfloat16 or wider, within the bound.
A program may use at most 64 MiB of HBM per device.

```python
import math
import jax
import jax.numpy as jnp
import numpy as np
from jax import lax

D = 2048
FF = 2816
TOK_DEV = 128
TOKENS = 4096
EXPERTS = 32
CAP = 16
N_SP = 32
N_TP = 8


def with_spikes(drawn, key, source, target, shards_of, factor):
    owner, partner = [(jnp.arange(drawn.shape[axis_at]) // (drawn.shape[axis_at] // shards_of)).reshape([-1 if axis == axis_at else 1 for axis in range(drawn.ndim)]) for axis_at in (source, target)]
    chosen = jax.random.permutation(key, shards_of)[partner]
    strong = (owner == chosen) | (owner == (partner + shards_of // 2) % shards_of)
    return jnp.where(strong, factor * drawn, drawn)


def block_levels(rng, shape, pieces, smallest, top_value):
    def one(axis_at, blocks):
        heights = jax.random.uniform(jax.random.fold_in(jax.random.fold_in(rng, 6), axis_at), (blocks,), jnp.float32, smallest / len(pieces), top_value / len(pieces))
        return jnp.repeat(jnp.exp(heights), shape[axis_at] // blocks).reshape((-1,) + (1,) * (len(shape) - axis_at - 1))

    level = one(*pieces[0])
    for cut in pieces[1:]:
        level = level * one(*cut)
    return level


def routed_block(key, own, number, rows, amount, top, bound, skew):
    order = jax.random.permutation(key, amount)
    crowded, ordinary = portions_of(amount, rows * top, bound, skew, True), portions_of(amount, rows * top, bound, skew, False)
    places = jnp.arange(amount)

    def named(sizes, rotation):
        used = int((sizes > 0).sum())
        fixed = max(1, used // 4)
        passed = fixed + (places - fixed + rotation * (used - fixed)) % max(1, amount - fixed)
        return jnp.zeros((amount,), jnp.int32).at[order[jnp.where(places < fixed, places, passed)]].set(jnp.asarray(sizes, jnp.int32))

    sizes = jnp.where(number % 4 == 0, named(crowded, number // 4), named(ordinary, number - number // 4 - 1))
    mixed = jax.random.permutation(jax.random.fold_in(own, 3), amount)
    donor, sink = mixed[0:amount // 2 * 2:2], mixed[1:amount // 2 * 2:2]
    room = jnp.minimum(sizes[donor] - 1, bound - sizes[sink]) // 2
    room = jnp.where((donor == order[0]) | (sink == order[0]) | (sizes[sink] == 0), 0, jnp.maximum(room, 0))
    passed = jax.random.randint(jax.random.fold_in(own, 4), (amount // 2,), 0, 1 << 20) % (room + 1)
    sizes = sizes.at[donor].add(-passed).at[sink].add(passed)
    labels = jnp.searchsorted(jnp.cumsum(sizes), jnp.arange(rows * top), side="right").astype(jnp.int32)
    grid = labels.reshape(top, rows).T
    grid = grid[jax.random.permutation(jax.random.fold_in(own, 1), rows)]
    rotation = jax.random.randint(jax.random.fold_in(own, 2), (rows, 1), 0, top)
    return jnp.take_along_axis(grid, (jnp.arange(top)[None, :] + rotation) % top, axis=1)


def portions_of(count, total, most, skew, full):
    weights = [(1 << 20) // math.isqrt(standing ** skew) + 1 for standing in range(1, count + 1)]
    largest = most if full else min(most, max(-(-total // count), total * weights[0] // sum(weights)))
    least = 1 if total - largest >= count - 1 else 0
    given, surplus = [largest] + [least] * (count - 1), total - largest - least * (count - 1)
    while surplus > 0:
        movable = [i for i in range(1, count) if given[i] < largest] or [i for i in range(1, count) if given[i] < most]
        mass, left = sum([weights[i] for i in movable]), surplus
        for i in movable:
            addition = min(most - given[i], max(1, left * weights[i] // mass), surplus)
            given[i] = given[i] + addition
            surplus = surplus - addition
    return np.array(given)


def normal_values(rng, shape, deviation, reach, split=(), kind=jnp.bfloat16):
    loudness = block_levels(rng, shape, split, -0.22, 0.18) if split else 1.0
    values = jax.random.normal(rng, shape, jnp.float32) * deviation * loudness
    return jnp.minimum(jnp.maximum(values, -reach), reach).astype(kind)


def bell_draw_with(rng, extent, spread, limit, pieces, heavy, held_as=jnp.bfloat16):
    array = spread * jax.random.normal(rng, extent, jnp.float32)
    if pieces:
        array = array * block_levels(rng, extent, pieces, -0.22, 0.18)
    return jnp.clip(with_spikes(array, jax.random.fold_in(rng, 3), *heavy), -limit, limit).astype(held_as)


def setup_inputs(seed: int = 0) -> dict:
    arg_keys = jax.random.split(jax.random.key(seed), 14)
    out_grad = bell_draw_with(arg_keys[0], (TOKENS, D), 1.0, 6.0, ((0, 32), (1, 8)), (0, 1, 32, 2.75))
    moe_input = normal_values(arg_keys[1], (TOKENS, D), 1.0, 6.0, ((0, 32), (1, 8)))
    route_weight = jnp.clip(jnp.exp(math.log(1.0) - 1.609438 * jax.random.uniform(arg_keys[2], (TOKENS, 2), jnp.float32) ** block_levels(arg_keys[2], (TOKENS, 2), ((0, 32),), -0.2, 0.2)), 0.2, 1.0)
    route_ids_keys = jax.random.split(jax.random.fold_in(arg_keys[3], 1), TOKENS // TOK_DEV)
    route_ids_turns = jax.random.permutation(jax.random.fold_in(arg_keys[3], 3), TOKENS // TOK_DEV)
    route_ids = jax.vmap(lambda own, number: routed_block(jax.random.fold_in(arg_keys[3], 2), own, number, TOK_DEV, EXPERTS, 2, CAP, 1))(route_ids_keys, route_ids_turns).reshape((TOKENS, 2))
    gate_proj = normal_values(arg_keys[4], (EXPERTS, D, FF), D ** -0.5, 0.125, ((0, 32), (2, 8)))
    up_proj = normal_values(arg_keys[5], (EXPERTS, D, FF), D ** -0.5, 0.125, ((0, 32), (2, 8)))
    down_proj = normal_values(arg_keys[6], (EXPERTS, FF, D), FF ** -0.5, 0.109375, ((0, 32), (1, 8)))
    out_proj = normal_values(arg_keys[7], (D, D), D ** -0.5, 0.125, ((1, 8),))
    conv_out = normal_values(arg_keys[8], (TOKENS, D), 1.0, 6.0, ((0, 32), (1, 8)))
    gate_b = normal_values(arg_keys[9], (TOKENS, D), 1.0, 6.0, ((0, 32), (1, 8)))
    gate_c = normal_values(arg_keys[10], (TOKENS, D), 1.0, 6.0, ((0, 32), (1, 8)))
    value_v = normal_values(arg_keys[11], (TOKENS, D), 1.0, 6.0, ((0, 32), (1, 8)))
    conv_taps = normal_values(arg_keys[12], (3, D), 0.6, 3.0, ((1, 8),), jnp.float32)
    return {"out_grad": out_grad, "moe_input": moe_input, "route_weight": route_weight, "route_ids": route_ids, "gate_proj": gate_proj, "up_proj": up_proj, "down_proj": down_proj, "out_proj": out_proj, "conv_out": conv_out, "gate_b": gate_b, "gate_c": gate_c, "value_v": value_v, "conv_taps": conv_taps}


def slot_table(route_ids):
    flat = route_ids.reshape(N_SP, TOK_DEV * 2).astype(jnp.int32)
    onehot = (flat[:, :, None] == jnp.arange(EXPERTS, dtype=jnp.int32)[None, None, :]).astype(jnp.int32)
    before = jnp.cumsum(onehot, axis=1) - onehot
    slot = jnp.sum(before * onehot, axis=2).astype(jnp.int32)
    return (flat * CAP + slot).astype(jnp.int32)


def place_rows(rows, index):
    return jnp.zeros((EXPERTS * CAP, rows.shape[1]), rows.dtype).at[index].set(rows)


def reference(out_grad, moe_input, route_weight, route_ids, gate_proj, up_proj, down_proj, out_proj, conv_out, gate_b, gate_c, value_v, conv_taps):
    dest = slot_table(route_ids)
    sent = (route_weight[:, :, None] * out_grad.astype(jnp.float32)[:, None, :]).astype(jnp.bfloat16)
    rows_x = jnp.broadcast_to(moe_input[:, None, :], (TOKENS, 2, D)).reshape(N_SP, 2 * TOK_DEV, D)
    rows_dy = sent.reshape(N_SP, 2 * TOK_DEV, D)
    slots_x = jax.vmap(place_rows)(rows_x, dest).reshape(N_SP, EXPERTS, CAP, D)
    slots_dy = jax.vmap(place_rows)(rows_dy, dest).reshape(N_SP, EXPERTS, CAP, D)
    width = FF // N_TP

    def expert(index):
        xin = slots_x[:, index].reshape(N_SP * CAP, D)
        dyin = slots_dy[:, index].reshape(N_SP * CAP, D)
        w_gate = gate_proj[index]
        w_up = up_proj[index]
        w_down = down_proj[index]
        gate = jnp.dot(xin, w_gate, preferred_element_type=jnp.float32)
        upval = jnp.dot(xin, w_up, preferred_element_type=jnp.float32)
        sig = jax.nn.sigmoid(gate)
        act = gate * sig
        hidden = (act * upval).astype(jnp.bfloat16)
        g_down = jnp.dot(hidden.T, dyin, preferred_element_type=jnp.float32).astype(jnp.bfloat16)
        dhid = jnp.dot(dyin, w_down.T, preferred_element_type=jnp.float32)
        dgate = (dhid * upval * (sig * (1.0 + gate * (1.0 - sig)))).astype(jnp.bfloat16)
        dup = (dhid * act).astype(jnp.bfloat16)
        g_gate = jnp.dot(xin.T, dgate, preferred_element_type=jnp.float32).astype(jnp.bfloat16)
        g_up = jnp.dot(xin.T, dup, preferred_element_type=jnp.float32).astype(jnp.bfloat16)
        rows = N_SP * CAP
        part = jnp.einsum('rpf,dpf->prd', dgate.reshape(rows, N_TP, width).astype(jnp.float32),
                          w_gate.reshape(D, N_TP, width).astype(jnp.float32))
        part = part + jnp.einsum('rpf,dpf->prd', dup.reshape(rows, N_TP, width).astype(jnp.float32),
                                 w_up.reshape(D, N_TP, width).astype(jnp.float32))
        part = lax.optimization_barrier(part.astype(jnp.bfloat16)).astype(jnp.float32)
        back = jnp.sum(part, axis=0).astype(jnp.bfloat16)
        return g_gate, g_up, g_down, back

    grad_gate, grad_up, grad_down, backs = lax.map(expert, jnp.arange(EXPERTS, dtype=jnp.int32))
    backs = backs.reshape(EXPERTS, N_SP, CAP, D).transpose(1, 0, 2, 3).reshape(N_SP, EXPERTS * CAP, D)
    picked = jax.vmap(lambda table, index: table[index])(backs, dest)
    moe_grad = jnp.sum(picked.reshape(TOKENS, 2, D).astype(jnp.float32), axis=1)
    grad_h = (out_grad.astype(jnp.float32) + moe_grad).astype(jnp.bfloat16)
    grad_z = jnp.dot(grad_h, out_proj, preferred_element_type=jnp.float32)
    dconv = (grad_z * gate_b.astype(jnp.float32)).astype(jnp.bfloat16)
    grad_b = (grad_z * conv_out.astype(jnp.float32)).astype(jnp.bfloat16)
    padded = jnp.pad(dconv.astype(jnp.float32), ((1, 1), (0, 0)))
    grad_u = conv_taps[0] * padded[2:] + conv_taps[1] * padded[1:-1] + conv_taps[2] * padded[:-2]
    grad_c = (grad_u * value_v.astype(jnp.float32)).astype(jnp.bfloat16)
    grad_v = (grad_u * gate_c.astype(jnp.float32)).astype(jnp.bfloat16)
    mixed = (gate_b.astype(jnp.float32) * conv_out.astype(jnp.float32)).astype(jnp.bfloat16)
    grad_out = jnp.dot(grad_h.T, mixed, preferred_element_type=jnp.float32)
    return grad_gate, grad_up, grad_down, grad_out, grad_b, grad_c, grad_v
```

```python
import jax
import jax.numpy as jnp
from jax import lax
from jax.experimental import pallas as pl
from jax.experimental.pallas import tpu as pltpu
from jax.sharding import PartitionSpec as P

MESH = pl.DeviceIdType.MESH
BF = jnp.bfloat16
F32 = jnp.float32
NZ, NX, NY = 8, 4, 4
NSP = NZ * NX
CAP = 16
TOK = 128
CH = 256
D = 2048
FFL = 352
OFF = 384
ROWS = NSP * CAP
CHUNKS = 4
CR = ROWS // CHUNKS


def dot(a, b, ca, cb):
    return lax.dot_general(a, b, (((ca,), (cb,)), ((), ())), preferred_element_type=F32)


def offset_of(k):
    odd = k % 2
    return odd * ((k + 1) // 2) + (1 - odd) * ((NZ - k // 2) % NZ)


def kernel(
    out_grad,
    moe_input,
    route_weight,
    ids_t,
    gate_proj,
    up_proj,
    down_proj,
    out_proj,
    conv_out,
    gate_b,
    gate_c,
    value_v,
    taps,
    g_gate,
    g_up,
    g_down,
    g_out,
    g_b,
    g_c,
    g_v,
    send,
    xd,
    wg,
    wu,
    wd,
    wo,
    place,
    dgu,
    hid_t,
    part,
    sib,
    ssum,
    rl,
    rr,
    fl,
    fr,
    rsum,
    ret,
    hf,
    js,
    dt,
    mx,
    hsend,
    halo,
    og_gate,
    og_up,
    og_down,
    w_sem,
    o_sem,
    a_send,
    a_recv,
    b_send,
    b_recv,
    d_send,
    d_recv,
    e_send,
    e_recv,
    h_send,
    h_recv,
    j_send,
    j_recv,
    k_send,
    k_recv,
    m_send,
    m_recv,
    n_send,
    n_recv,
):
    s = lax.axis_index("sp")
    t = lax.axis_index("tp")
    z, x = s // NX, s % NX
    y, c = t // 2, t % 2
    up, down, far = (y + 1) % NY, (y + NY - 1) % NY, (y + 2) % NY
    t_up, t_down, t_sib = up * 2 + c, down * 2 + c, y * 2 + (1 - c)
    t_far = far * 2 + c

    def remote(src, dst, ssem, rsem, sp, tp):
        return pltpu.make_async_remote_copy(
            src_ref=src,
            dst_ref=dst,
            send_sem=ssem,
            recv_sem=rsem,
            device_id={"sp": sp, "tp": tp},
            device_id_type=MESH,
        )

    def arrived(ref, rsem):
        remote(ref, ref, n_send.at[0], rsem, s, t).wait_recv()

    def left(ref, ssem):
        remote(ref, ref, ssem, n_recv.at[0], s, t).wait_send()

    barrier = pltpu.get_barrier_semaphore()

    def greet(i, carry):
        pl.semaphore_signal(
            barrier, inc=1, device_id={"sp": (s + i) % NSP, "tp": t}, device_id_type=MESH
        )
        return carry

    lax.fori_loop(1, NSP, greet, 0)
    for peer in (t_up, t_down, t_sib):
        pl.semaphore_signal(barrier, inc=1, device_id={"sp": s, "tp": peer}, device_id_type=MESH)
    for j in range(NX):

        @pl.when(jnp.logical_not(jnp.logical_and(z == t, x == j)))
        def _():
            pl.semaphore_signal(
                barrier, inc=1, device_id={"sp": t * NX + j, "tp": z}, device_id_type=MESH
            )

    loads = [
        pltpu.make_async_copy(gate_proj.at[0], wg, w_sem.at[0]),
        pltpu.make_async_copy(up_proj.at[0], wu, w_sem.at[1]),
        pltpu.make_async_copy(down_proj.at[0], wd, w_sem.at[2]),
        pltpu.make_async_copy(out_proj, wo, w_sem.at[3]),
    ]
    for load in loads:
        load.start()

    ids = ids_t[...]
    experts = lax.broadcasted_iota(jnp.int32, (NSP, TOK), 0)
    e0 = jnp.where(experts == ids[0:1, :], 1.0, 0.0).astype(F32)
    e1 = jnp.where(experts == ids[1:2, :], 1.0, 0.0).astype(F32)
    row = lax.broadcasted_iota(jnp.int32, (TOK, TOK), 0)
    col = lax.broadcasted_iota(jnp.int32, (TOK, TOK), 1)
    earlier = jnp.where(row < col, 1.0, 0.0).astype(BF)
    before = dot((e0 + e1).astype(BF), earlier, 1, 0)
    slot0 = jnp.sum(before * e0, axis=0, keepdims=True)
    slot1 = jnp.sum(before * e1, axis=0, keepdims=True)
    idf = ids.astype(F32) * CAP
    at = lax.broadcasted_iota(jnp.int32, (ROWS, TOK), 0).astype(F32)
    p0 = jnp.where(at == idf[0:1, :] + slot0, 1.0, 0.0).astype(BF)
    p1 = jnp.where(at == idf[1:2, :] + slot1, 1.0, 0.0).astype(BF)
    place[...] = p0 + p1
    og = out_grad[...].astype(F32)
    w = route_weight[...]
    dy0 = (w[:, 0:1] * og).astype(BF)
    dy1 = (w[:, 1:2] * og).astype(BF)
    send[0] = dot(p0 + p1, moe_input[...], 1, 0).astype(BF)
    send[1] = (dot(p0, dy0, 1, 0) + dot(p1, dy1, 1, 0)).astype(BF)
    mixed = (gate_b[...].astype(F32) * conv_out[...].astype(F32)).astype(BF)
    own_rows = pl.ds(pl.multiple_of(s * TOK, TOK), TOK)
    mx[own_rows, :] = mixed
    dgu[...] = jnp.zeros_like(dgu)

    def cols(tp, width=CH):
        return pl.ds(pl.multiple_of(tp * width, width), width)

    pl.semaphore_wait(barrier, NSP - 1 + 3 + 4 - jnp.where(z == t, 1, 0))

    def a_copy(i):
        k, dx = i // NX, i % NX
        target = ((z + offset_of(k)) % NZ) * NX + (x + dx) % NX
        src = send.at[:, pl.ds(pl.multiple_of(target * CAP, CAP), CAP), :]
        dst = xd.at[:, pl.ds(pl.multiple_of(k * NX * CAP + x * CAP, CAP), CAP), cols(t)]
        return remote(src, dst, a_send.at[i], a_recv.at[k * NX + x], target, t)

    def a_start(i, carry):
        a_copy(i).start()
        return carry

    lax.fori_loop(1, NSP, a_start, 0)
    here = pl.ds(pl.multiple_of(x * CAP, CAP), CAP)
    xd[:, here, cols(t)] = send[:, pl.ds(pl.multiple_of(s * CAP, CAP), CAP), :]

    x_peers = [(1, (x + 1) % NX, (x + 3) % NX), (3, (x + 3) % NX, (x + 1) % NX), (2, (x + 2) % NX, (x + 2) % NX)]
    for i, (_, to, _from) in enumerate(x_peers):
        remote(
            mx.at[own_rows, :], mx.at[own_rows, :], m_send.at[i], m_recv.at[i], z * NX + to, t
        ).start()

    def a_wait(k, first):
        def body(i, carry):
            xx = (x + i) % NX
            arrived(
                xd.at[:, pl.ds(pl.multiple_of(k * NX * CAP + xx * CAP, CAP), CAP), cols(t)],
                a_recv.at[k * NX + xx],
            )
            return carry

        lax.fori_loop(first, NX, body, 0)

    def gather(piece, ss, rs):
        def one():
            remote(piece(t), piece(t), ss(0), rs(0), s, t_up).start()
            remote(piece(t), piece(t), ss(1), rs(1), s, t_down).start()
            remote(piece(t), piece(t), ss(4), rs(4), s, t_sib).start()

        def two():
            arrived(piece(t_down), rs(0))
            remote(piece(t_down, 0), piece(t_down, 0), ss(2), rs(2), s, t_up).start()
            remote(piece(t_down), piece(t_down), ss(5), rs(5), s, t_sib).start()
            arrived(piece(t_up), rs(1))
            remote(piece(t_up, 1), piece(t_up, 1), ss(3), rs(3), s, t_down).start()
            remote(piece(t_up), piece(t_up), ss(6), rs(6), s, t_sib).start()

        def three():
            arrived(piece(t_far, 0), rs(2))
            remote(piece(t_far, 0), piece(t_far, 0), ss(7), rs(7), s, t_sib).start()
            arrived(piece(t_far, 1), rs(3))
            remote(piece(t_far, 1), piece(t_far, 1), ss(8), rs(8), s, t_sib).start()

        def four():
            arrived(piece(t_sib), rs(4))
            arrived(piece(down * 2 + 1 - c), rs(5))
            arrived(piece(up * 2 + 1 - c), rs(6))
            arrived(piece(far * 2 + 1 - c, 0), rs(7))
            arrived(piece(far * 2 + 1 - c, 1), rs(8))

        def end():
            for i in (0, 1, 4, 5, 6):
                left(piece(t), ss(i))
            left(piece(t, 0), ss(2))
            left(piece(t, 1), ss(3))
            left(piece(t, 0), ss(7))
            left(piece(t, 1), ss(8))

        return one, two, three, four, end

    def chunk_piece(m):
        rows = pl.ds(m * CR, CR)

        def piece(tp, half=None):
            if half is None:
                return xd.at[:, rows, cols(tp)]
            return xd.at[half, rows, cols(tp)]

        return piece

    chunk = [
        gather(
            chunk_piece(m),
            lambda i, m=m: b_send.at[m * 9 + i],
            lambda i, m=m: b_recv.at[m * 9 + i],
        )
        for m in range(CHUNKS)
    ]

    def plane(zz, half=None):
        base = zz * (NX * TOK)
        if half is None:
            return mx.at[pl.ds(pl.multiple_of(base, NX * TOK), NX * TOK), :]
        return mx.at[pl.ds(pl.multiple_of(base + half * 2 * TOK, 2 * TOK), 2 * TOK), :]

    z_up, z_down = ((z + 1) % NZ) * NX + x, ((z + NZ - 1) % NZ) * NX + x

    def hop(r):
        if r == 1:
            for i, (_, _to, source) in enumerate(x_peers):
                arrived(
                    mx.at[pl.ds(pl.multiple_of((z * NX + source) * TOK, TOK), TOK), :],
                    m_recv.at[i],
                )
        else:
            arrived(plane((z + NZ - (r - 1)) % NZ), n_recv.at[2 * r - 2])
            arrived(plane((z + r - 1) % NZ), n_recv.at[2 * r - 1])
        low, high = (0, 1) if r == 4 else (None, None)
        a = plane((z + NZ - (r - 1)) % NZ, low)
        b = plane((z + r - 1) % NZ, high)
        remote(a, a, n_send.at[2 * r], n_recv.at[2 * r], z_up, t).start()
        remote(b, b, n_send.at[2 * r + 1], n_recv.at[2 * r + 1], z_down, t).start()

    for m in range(CHUNKS):
        a_wait(2 * m, 1 if m == 0 else 0)
        a_wait(2 * m + 1, 0)
        chunk[m][0]()
        if m >= 1:
            chunk[m - 1][1]()
        if m >= 2:
            chunk[m - 2][2]()
    hop(1)
    chunk[3][1]()
    chunk[2][2]()
    chunk[3][2]()
    hop(2)
    for m in range(CHUNKS):
        chunk[m][3]()

    for load in loads:
        load.wait()
    half_rows = ROWS // 2
    for m in range(2):
        rows = pl.ds(m * half_rows, half_rows)
        xm = xd[0, rows, :]
        g = dot(xm, wg[...], 1, 0)
        u = dot(xm, wu[...], 1, 0)
        dh = dot(xd[1, rows, :], wd[...], 1, 1)
        sig = 1.0 / (1.0 + jnp.exp(-g))
        act = g * sig
        hid_t[:, rows] = (act * u).T.astype(BF)
        dgu[rows, 0:FFL] = (dh * u * (sig * (1.0 + g * (1.0 - sig)))).astype(BF)
        dgu[rows, OFF : OFF + FFL] = (dh * act).astype(BF)
    hop(3)

    def grads(lo, hi):
        def body(i, carry):
            cs = cols(i)
            gu = dot(xd[0, :, cs], dgu[...], 0, 0)
            og_gate[cs, :] = gu[:, 0:FFL].astype(BF)
            og_up[cs, :] = gu[:, OFF : OFF + FFL].astype(BF)
            og_down[:, cs] = dot(hid_t[...], xd[1, :, cs], 1, 0).astype(BF)
            return carry

        lax.fori_loop(lo, hi, body, 0)

    def dx(m):
        rows = pl.ds(m * CR, CR)
        dg = dgu[rows, 0:FFL]
        du = dgu[rows, OFF : OFF + FFL]

        def body(i, carry):
            cs = cols(i)
            part[i % 2, i // 2, rows, :] = (
                dot(dg, wg[cs, :], 1, 1) + dot(du, wu[cs, :], 1, 1)
            ).astype(BF)
            return carry

        lax.fori_loop(0, 8, body, 0)

    def d_rows(m):
        return pl.ds(m * CR, CR)

    def d_low(m):
        return pl.ds(m * CR, CR // 2)

    def d_high(m):
        return pl.ds(m * CR + CR // 2, CR // 2)

    def d_half(m):
        return pl.ds(m * (CR // 2), CR // 2)

    def d0(m):
        remote(
            part.at[1 - c, :, d_rows(m), :],
            sib.at[:, d_rows(m), :],
            d_send.at[m * 5],
            d_recv.at[m * 5],
            s,
            t_sib,
        ).start()

    def d1(m):
        arrived(sib.at[:, d_rows(m), :], d_recv.at[m * 5])
        ssum[:, d_rows(m), :] = (
            part[c, :, d_rows(m), :].astype(F32) + sib[:, d_rows(m), :].astype(F32)
        ).astype(BF)
        remote(
            ssum.at[far, d_low(m), :],
            rl.at[d_half(m), :],
            d_send.at[m * 5 + 1],
            d_recv.at[m * 5 + 1],
            s,
            t_up,
        ).start()
        remote(
            ssum.at[far, d_high(m), :],
            rr.at[d_half(m), :],
            d_send.at[m * 5 + 2],
            d_recv.at[m * 5 + 2],
            s,
            t_down,
        ).start()

    def d2(m):
        arrived(rl.at[d_half(m), :], d_recv.at[m * 5 + 1])
        ssum[up, d_low(m), :] = (
            ssum[up, d_low(m), :].astype(F32) + rl[d_half(m), :].astype(F32)
        ).astype(BF)
        remote(
            ssum.at[up, d_rows(m), :],
            fl.at[d_rows(m), :],
            d_send.at[m * 5 + 3],
            d_recv.at[m * 5 + 3],
            s,
            t_up,
        ).start()
        arrived(rr.at[d_half(m), :], d_recv.at[m * 5 + 2])
        ssum[down, d_high(m), :] = (
            ssum[down, d_high(m), :].astype(F32) + rr[d_half(m), :].astype(F32)
        ).astype(BF)
        remote(
            ssum.at[down, d_rows(m), :],
            fr.at[d_rows(m), :],
            d_send.at[m * 5 + 4],
            d_recv.at[m * 5 + 4],
            s,
            t_down,
        ).start()

    def e_copy(k, xx):
        target = ((z + NZ - offset_of(k)) % NZ) * NX + xx
        i = k * NX + xx
        return remote(
            rsum.at[pl.ds(pl.multiple_of(i * CAP, CAP), CAP), :],
            ret.at[pl.ds(pl.multiple_of(s * CAP, CAP), CAP), :],
            e_send.at[i],
            e_recv.at[s],
            target,
            t,
        )

    def d3(m):
        arrived(fl.at[d_rows(m), :], d_recv.at[m * 5 + 3])
        arrived(fr.at[d_rows(m), :], d_recv.at[m * 5 + 4])
        rsum[d_rows(m), :] = (
            ssum[y, d_rows(m), :].astype(F32)
            + fl[d_rows(m), :].astype(F32)
            + fr[d_rows(m), :].astype(F32)
        ).astype(BF)

        def start(k, first):
            def body(i, carry):
                e_copy(k, (x + i) % NX).start()
                return carry

            lax.fori_loop(first, NX, body, 0)

        start(2 * m + 1, 0)
        start(2 * m, 1 if m == 0 else 0)
        if m == 0:
            ret[pl.ds(pl.multiple_of(s * CAP, CAP), CAP), :] = rsum[here, :]

    dx(3)
    d0(3)
    dx(2)
    d0(2)
    d1(3)
    dx(1)
    d0(1)
    d1(2)
    d2(3)
    dx(0)
    d0(0)
    d1(1)
    d2(2)
    grads(0, 2)
    d3(3)
    d1(0)
    d2(1)
    grads(2, 4)
    d3(2)
    d2(0)
    hop(4)
    d3(1)
    grads(4, 6)
    d3(0)
    grads(6, 8)
    stores = [
        pltpu.make_async_copy(og_gate, g_gate.at[0], o_sem.at[0]),
        pltpu.make_async_copy(og_up, g_up.at[0], o_sem.at[1]),
        pltpu.make_async_copy(og_down, g_down.at[0], o_sem.at[2]),
    ]
    for store in stores:
        store.start()

    def e_wait(i, carry):
        e = (s + i) % NSP
        arrived(ret.at[pl.ds(pl.multiple_of(e * CAP, CAP), CAP), :], e_recv.at[e])
        return carry

    lax.fori_loop(1, NSP, e_wait, 0)

    dh = out_grad[...].astype(F32) + dot(place[...], ret[...], 0, 0)
    js[...] = dh.T.astype(BF)
    hf[:, cols(t)] = dh.astype(BF)

    own_cols = pl.ds(pl.multiple_of(s * TOK, TOK), TOK)
    for j in range(NX):
        mine = jnp.logical_and(z == t, x == j)

        @pl.when(jnp.logical_not(mine))
        def _():
            remote(
                js.at[pl.ds(64 * j, 64), :],
                dt.at[:, own_cols],
                j_send.at[j],
                j_recv.at[x],
                t * NX + j,
                z,
            ).start()

        @pl.when(mine)
        def _():
            dt[:, own_cols] = js[pl.ds(64 * j, 64), :]

    def h_piece(tp, half=None):
        if half is None:
            return hf.at[:, cols(tp)]
        return hf.at[pl.ds(half * 64, 64), cols(tp)]

    def j_piece(tp, half=None):
        if half is None:
            return dt.at[:, cols(tp, 512)]
        return dt.at[pl.ds(half * 32, 32), cols(tp, 512)]

    hg = gather(h_piece, lambda i: h_send.at[i], lambda i: h_recv.at[i])
    jg = gather(j_piece, lambda i: k_send.at[i], lambda i: k_recv.at[i])
    hg[0]()
    hg[1]()
    for j in range(NX):

        @pl.when(jnp.logical_not(jnp.logical_and(z == t, x == j)))
        def _():
            arrived(
                dt.at[:, pl.ds(pl.multiple_of(t * 512 + j * TOK, TOK), TOK)], j_recv.at[j]
            )

    jg[0]()
    hg[2]()
    hg[3]()
    dz = dot(hf[...], wo[...], 1, 0)
    dconv = (dz * gate_b[...].astype(F32)).astype(BF)
    hsend[...] = dconv

    @pl.when(s < NSP - 1)
    def _():
        remote(
            hsend.at[pl.ds(TOK - 16, 16), :], halo.at[0], j_send.at[4], j_recv.at[4], s + 1, t
        ).start()

    @pl.when(s > 0)
    def _():
        remote(hsend.at[pl.ds(0, 16), :], halo.at[1], j_send.at[5], j_recv.at[5], s - 1, t).start()

    jg[1]()
    g_b[...] = (dz * conv_out[...].astype(F32)).astype(BF)
    jg[2]()

    @pl.when(s > 0)
    def _():
        arrived(halo.at[0], j_recv.at[4])

    @pl.when(s == 0)
    def _():
        halo[0] = jnp.zeros((16, CH), BF)

    @pl.when(s < NSP - 1)
    def _():
        arrived(halo.at[1], j_recv.at[5])

    @pl.when(s == NSP - 1)
    def _():
        halo[1] = jnp.zeros((16, CH), BF)

    d = dconv.astype(F32)
    at_row = lax.broadcasted_iota(jnp.int32, (TOK, CH), 0)
    before_first = halo[0].astype(F32)[15:16, :]
    after_last = halo[1].astype(F32)[0:1, :]
    earlier_rows = jnp.where(at_row == 0, before_first, pltpu.roll(d, 1, 0))
    later_rows = jnp.where(at_row == TOK - 1, after_last, pltpu.roll(d, TOK - 1, 0))
    tp3 = taps[...]
    grad_u = tp3[0:1, :] * later_rows + tp3[1:2, :] * d + tp3[2:3, :] * earlier_rows
    g_c[...] = (grad_u * value_v[...].astype(F32)).astype(BF)
    g_v[...] = (grad_u * gate_c[...].astype(F32)).astype(BF)

    arrived(plane((z + 4) % NZ, 0), n_recv.at[8])
    arrived(plane((z + 4) % NZ, 1), n_recv.at[9])
    jg[3]()
    g_out[...] = dot(dt[...], mx[...], 1, 0)

    def a_left(i, carry):
        a_copy(i).wait_send()
        return carry

    lax.fori_loop(1, NSP, a_left, 0)
    for m in range(CHUNKS):
        chunk[m][4]()
        left(part.at[0, :, d_rows(m), :], d_send.at[m * 5])
        left(rl.at[d_half(m), :], d_send.at[m * 5 + 1])
        left(rr.at[d_half(m), :], d_send.at[m * 5 + 2])
        left(fl.at[d_rows(m), :], d_send.at[m * 5 + 3])
        left(fr.at[d_rows(m), :], d_send.at[m * 5 + 4])

    def e_left(i, carry):
        e_copy(i // NX, (x + i % NX) % NX).wait_send()
        return carry

    lax.fori_loop(1, NSP, e_left, 0)
    hg[4]()
    jg[4]()
    for i in range(3):
        left(mx.at[own_rows, :], m_send.at[i])
    for r in range(1, 5):
        half = 0 if r == 4 else None
        left(plane(z, half), n_send.at[2 * r])
        left(plane(z, half), n_send.at[2 * r + 1])
    for j in range(NX):

        @pl.when(jnp.logical_not(jnp.logical_and(z == t, x == j)))
        def _():
            left(js.at[pl.ds(64 * j, 64), :], j_send.at[j])

    @pl.when(s < NSP - 1)
    def _():
        left(halo.at[0], j_send.at[4])

    @pl.when(s > 0)
    def _():
        left(halo.at[1], j_send.at[5])

    for store in stores:
        store.wait()


def local(
    out_grad,
    moe_input,
    route_weight,
    route_ids,
    gate_proj,
    up_proj,
    down_proj,
    out_proj,
    conv_out,
    gate_b,
    gate_c,
    value_v,
    conv_taps,
):
    vm = pl.BlockSpec(memory_space=pltpu.VMEM)
    hbm = pl.BlockSpec(memory_space=pl.ANY)
    dma = pltpu.SemaphoreType.DMA
    shape = jax.ShapeDtypeStruct
    return pl.pallas_call(
        kernel,
        out_shape=(
            shape((1, D, FFL), BF),
            shape((1, D, FFL), BF),
            shape((1, FFL, D), BF),
            shape((64, CH), F32),
            shape((TOK, CH), BF),
            shape((TOK, CH), BF),
            shape((TOK, CH), BF),
        ),
        in_specs=[vm, vm, vm, vm, hbm, hbm, hbm, hbm, vm, vm, vm, vm, vm],
        out_specs=(hbm, hbm, hbm, vm, vm, vm, vm),
        scratch_shapes=[
            pltpu.VMEM((2, ROWS, CH), BF),
            pltpu.VMEM((2, ROWS, D), BF),
            pltpu.VMEM((D, FFL), BF),
            pltpu.VMEM((D, FFL), BF),
            pltpu.VMEM((FFL, D), BF),
            pltpu.VMEM((D, CH), BF),
            pltpu.VMEM((ROWS, TOK), BF),
            pltpu.VMEM((ROWS, 2 * OFF), BF),
            pltpu.VMEM((FFL, ROWS), BF),
            pltpu.VMEM((2, NY, ROWS, CH), BF),
            pltpu.VMEM((NY, ROWS, CH), BF),
            pltpu.VMEM((NY, ROWS, CH), BF),
            pltpu.VMEM((ROWS // 2, CH), BF),
            pltpu.VMEM((ROWS // 2, CH), BF),
            pltpu.VMEM((ROWS, CH), BF),
            pltpu.VMEM((ROWS, CH), BF),
            pltpu.VMEM((ROWS, CH), BF),
            pltpu.VMEM((ROWS, CH), BF),
            pltpu.VMEM((TOK, D), BF),
            pltpu.VMEM((CH, TOK), BF),
            pltpu.VMEM((64, NSP * TOK), BF),
            pltpu.VMEM((NSP * TOK, CH), BF),
            pltpu.VMEM((TOK, CH), BF),
            pltpu.VMEM((2, 16, CH), BF),
            pltpu.VMEM((D, FFL), BF),
            pltpu.VMEM((D, FFL), BF),
            pltpu.VMEM((FFL, D), BF),
            dma((4,)),
            dma((3,)),
            dma((NSP,)),
            dma((NSP,)),
            dma((9 * CHUNKS,)),
            dma((9 * CHUNKS,)),
            dma((5 * CHUNKS,)),
            dma((5 * CHUNKS,)),
            dma((NSP,)),
            dma((NSP,)),
            dma((9,)),
            dma((9,)),
            dma((6,)),
            dma((6,)),
            dma((9,)),
            dma((9,)),
            dma((3,)),
            dma((3,)),
            dma((10,)),
            dma((10,)),
        ],
        compiler_params=pltpu.CompilerParams(
            collective_id=0, has_side_effects=True, vmem_limit_bytes=60 * 1024 * 1024
        ),
        name="layer",
    )(
        out_grad,
        moe_input,
        route_weight,
        route_ids.T,
        gate_proj,
        up_proj,
        down_proj,
        out_proj,
        conv_out,
        gate_b,
        gate_c,
        value_v,
        conv_taps,
    )


def solution(mesh):
    return jax.shard_map(
        local,
        mesh=mesh,
        in_specs=(
            P("sp", "tp"),
            P("sp", "tp"),
            P("sp", None),
            P("sp", None),
            P("sp", None, "tp"),
            P("sp", None, "tp"),
            P("sp", "tp", None),
            P(None, "tp"),
            P("sp", "tp"),
            P("sp", "tp"),
            P("sp", "tp"),
            P("sp", "tp"),
            P(None, "tp"),
        ),
        out_specs=(
            P("sp", None, "tp"),
            P("sp", None, "tp"),
            P("sp", "tp", None),
            P("sp", "tp"),
            P("sp", "tp"),
            P("sp", "tp"),
            P("sp", "tp"),
        ),
        check_vma=False,
    )
```

```python
import jax
import jax.numpy as jnp
from jax import lax
from jax.experimental import pallas as pl
from jax.experimental.pallas import tpu as pltpu
from jax.sharding import PartitionSpec as P

MESH = pl.DeviceIdType.MESH
BF = jnp.bfloat16
F32 = jnp.float32
NZ, NX, NY = 8, 4, 4
NSP = NZ * NX
CAP = 16
TOK = 128
CH = 256
D = 2048
FFL = 352
ROWS = NSP * CAP
NK = 8
CR = ROWS // NK
NP = 4
PR = ROWS // NP
ORDER = (0, 1, 7, 4, 3, 5, 2, 6)


def dot(a, b, ca, cb):
    return lax.dot_general(a, b, (((ca,), (cb,)), ((), ())), preferred_element_type=F32)


def kernel(
    out_grad_h,
    moe_input_h,
    weight_h,
    ids_h,
    gate_proj,
    up_proj,
    down_proj,
    out_proj_h,
    conv_out_h,
    gate_b_h,
    gate_c_h,
    value_v_h,
    taps_h,
    g_gate,
    g_up,
    g_down,
    g_out_h,
    g_b_h,
    g_c_h,
    g_v_h,
    out_grad,
    moe_input,
    weight_t,
    ids_t,
    out_proj,
    conv_out,
    gate_b,
    gate_c,
    value_v,
    taps,
    g_out,
    g_b,
    g_c,
    g_v,
    og_gu,
    og_down,
    i_sem,
    o_sem,
    send,
    xd,
    wgu,
    wd,
    place,
    dgu_t,
    hid_t,
    part,
    sib,
    ssum,
    along,
    rsum,
    ret,
    hf,
    js,
    dt,
    mx,
    hsend,
    halo,
    w_sem,
    a_send,
    a_recv,
    b_send,
    b_recv,
    d_send,
    d_recv,
    e_send,
    e_recv,
    h_send,
    h_recv,
    j_send,
    j_recv,
    k_send,
    k_recv,
    m_send,
    m_recv,
    n_send,
    n_recv,
):
    s = lax.axis_index("sp")
    t = lax.axis_index("tp")
    z, x = s // NX, s % NX
    y, c = t // 2, t % 2
    up, down, far = (y + 1) % NY, (y + NY - 1) % NY, (y + 2) % NY
    t_up, t_down, t_sib = up * 2 + c, down * 2 + c, y * 2 + (1 - c)
    t_far = far * 2 + c

    def remote(src, dst, ssem, rsem, sp, tp):
        return pltpu.make_async_remote_copy(
            src_ref=src,
            dst_ref=dst,
            send_sem=ssem,
            recv_sem=rsem,
            device_id={"sp": sp, "tp": tp},
            device_id_type=MESH,
        )

    def arrived(ref, rsem):
        remote(ref, ref, n_send.at[0], rsem, s, t).wait_recv()

    def left(ref, ssem):
        remote(ref, ref, ssem, n_recv.at[0], s, t).wait_send()

    barrier = pltpu.get_barrier_semaphore()

    def greet(i, carry):
        pl.semaphore_signal(
            barrier, inc=1, device_id={"sp": (s + i) % NSP, "tp": t}, device_id_type=MESH
        )
        return carry

    lax.fori_loop(1, NSP, greet, 0)
    for peer in (t_up, t_down, t_far, t_sib):
        pl.semaphore_signal(barrier, inc=1, device_id={"sp": s, "tp": peer}, device_id_type=MESH)
    for j in range(NX):

        @pl.when(jnp.logical_not(jnp.logical_and(z == t, x == j)))
        def _():
            pl.semaphore_signal(
                barrier, inc=1, device_id={"sp": t * NX + j, "tp": z}, device_id_type=MESH
            )

    small = [
        pltpu.make_async_copy(a, b, i_sem.at[i])
        for i, (a, b) in enumerate(
            (
                (ids_h, ids_t),
                (weight_h, weight_t),
                (out_grad_h, out_grad),
                (moe_input_h, moe_input),
                (gate_b_h, gate_b),
                (conv_out_h, conv_out),
                (gate_c_h, gate_c),
                (value_v_h, value_v),
                (taps_h, taps),
                (out_proj_h, out_proj),
            )
        )
    ]
    loads = [
        pltpu.make_async_copy(gate_proj.at[0], wgu.at[pl.ds(0, FFL), :], w_sem.at[0]),
        pltpu.make_async_copy(up_proj.at[0], wgu.at[pl.ds(FFL, FFL), :], w_sem.at[1]),
        pltpu.make_async_copy(down_proj.at[0], wd, w_sem.at[2]),
    ]
    for load in small:
        load.start()
    for load in loads:
        load.start()

    for load in small[:6]:
        load.wait()

    ids = ids_t[...]
    experts = lax.broadcasted_iota(jnp.int32, (NSP, TOK), 0)
    e0 = jnp.where(experts == ids[0:1, :], 1.0, 0.0).astype(F32)
    e1 = jnp.where(experts == ids[1:2, :], 1.0, 0.0).astype(F32)
    row = lax.broadcasted_iota(jnp.int32, (TOK, TOK), 0)
    col = lax.broadcasted_iota(jnp.int32, (TOK, TOK), 1)
    earlier = jnp.where(row < col, 1.0, 0.0).astype(BF)
    before = dot((e0 + e1).astype(BF), earlier, 1, 0)
    slot0 = jnp.sum(before * e0, axis=0, keepdims=True)
    slot1 = jnp.sum(before * e1, axis=0, keepdims=True)
    idf = ids.astype(F32) * CAP
    at = lax.broadcasted_iota(jnp.int32, (ROWS, TOK), 0).astype(F32)
    p0 = jnp.where(at == idf[0:1, :] + slot0, 1.0, 0.0).astype(BF)
    p1 = jnp.where(at == idf[1:2, :] + slot1, 1.0, 0.0).astype(BF)
    place[...] = p0 + p1
    og = out_grad[...].astype(F32)
    w = weight_t[...]
    w0 = jnp.broadcast_to(w[0:1, :], (TOK, TOK)).T
    w1 = jnp.broadcast_to(w[1:2, :], (TOK, TOK)).T
    dy0 = (jnp.concatenate([w0, w0], axis=1) * og).astype(BF)
    dy1 = (jnp.concatenate([w1, w1], axis=1) * og).astype(BF)
    send[0] = dot(p0 + p1, moe_input[...], 1, 0).astype(BF)
    send[1] = (dot(p0, dy0, 1, 0) + dot(p1, dy1, 1, 0)).astype(BF)
    mixed = (gate_b[...].astype(F32) * conv_out[...].astype(F32)).astype(BF)
    own_rows = pl.ds(pl.multiple_of(s * TOK, TOK), TOK)
    mx[own_rows, :] = mixed

    def cols(tp, width=CH):
        return pl.ds(pl.multiple_of(tp * width, width), width)

    pl.semaphore_wait(barrier, NSP - 1 + 4 + 4 - jnp.where(z == t, 1, 0))

    def a_copy(k, xx):
        target = ((z + ORDER[k]) % NZ) * NX + xx
        src = send.at[:, pl.ds(pl.multiple_of(target * CAP, CAP), CAP), :]
        dst = xd.at[:, pl.ds(pl.multiple_of(k * CR + x * CAP, CAP), CAP), cols(t)]
        return remote(src, dst, a_send.at[k * NX + xx], a_recv.at[k * NX + x], target, t)

    def each_x(first, do):
        def body(i, carry):
            do((x + i) % NX)
            return carry

        lax.fori_loop(first, NX, body, 0)

    def a_start(k):
        each_x(1 if k == 0 else 0, lambda xx: a_copy(k, xx).start())

    def a_wait(k):
        def one(xx):
            arrived(
                xd.at[:, pl.ds(pl.multiple_of(k * CR + xx * CAP, CAP), CAP), cols(t)],
                a_recv.at[k * NX + xx],
            )

        each_x(1 if k == 0 else 0, one)

    here = pl.ds(pl.multiple_of(x * CAP, CAP), CAP)

    def gather(piece, ss, rs):
        def one():
            for i, peer in enumerate((t_sib, t_up, t_down, t_far)):
                remote(piece(t), piece(t), ss(i), rs(i), s, peer).start()

        def two():
            for i, origin in enumerate((t_down, t_up, t_far)):
                arrived(piece(origin), rs(1 + i))
                remote(piece(origin), piece(origin), ss(4 + i), rs(4 + i), s, t_sib).start()

        def three():
            for i, origin in enumerate((y, down, up, far)):
                arrived(piece(origin * 2 + 1 - c), rs(i if i == 0 else 3 + i))

        def end():
            for i in range(7):
                left(piece(t), ss(i))

        return one, two, three, end

    def relay(piece, ss, rs):
        def one():
            for i, peer in enumerate((t_sib, t_up, t_down)):
                remote(piece(t), piece(t), ss(i), rs(i), s, peer).start()

        def two():
            for i, (origin, peer) in enumerate(((t_down, t_up), (t_up, t_down))):
                arrived(piece(origin), rs(1 + i))
                half = piece(origin, i)
                remote(half, half, ss(3 + i), rs(3 + i), s, peer).start()
                remote(piece(origin), piece(origin), ss(5 + i), rs(5 + i), s, t_sib).start()

        def three():
            for i in range(2):
                half = piece(t_far, i)
                arrived(half, rs(3 + i))
                remote(half, half, ss(7 + i), rs(7 + i), s, t_sib).start()

        def four():
            arrived(piece(t_sib), rs(0))
            arrived(piece(down * 2 + 1 - c), rs(5))
            arrived(piece(up * 2 + 1 - c), rs(6))
            arrived(piece(far * 2 + 1 - c, 0), rs(7))
            arrived(piece(far * 2 + 1 - c, 1), rs(8))

        def end():
            for i in range(9):
                left(piece(t) if i in (0, 1, 2, 5, 6) else piece(t, 0), ss(i))

        return one, two, three, four, end

    def chunk_piece(k):
        rows = pl.ds(k * CR, CR)

        def piece(tp, half=None):
            if half is None:
                return xd.at[:, rows, cols(tp)]
            return xd.at[half, rows, cols(tp)]

        return piece

    chunk = [
        relay(
            chunk_piece(k),
            lambda i, k=k: b_send.at[k * 9 + i],
            lambda i, k=k: b_recv.at[k * 9 + i],
        )
        for k in range(NK)
    ]

    def block(zz, xx, half=None):
        base = (zz * NX + xx) * TOK
        if half is None:
            return mx.at[pl.ds(pl.multiple_of(base, TOK), TOK), :]
        return mx.at[pl.ds(pl.multiple_of(base + half * (TOK // 2), TOK // 2), TOK // 2), :]

    z_up, z_down = ((z + 1) % NZ) * NX + x, ((z + NZ - 1) % NZ) * NX + x
    x_up, x_down, x_far = (x + 1) % NX, (x + NX - 1) % NX, (x + 2) % NX

    def z_hop(r):
        low, high = (0, 1) if r == 4 else (None, None)
        a = block((z + NZ - (r - 1)) % NZ, x, low)
        b = block((z + r - 1) % NZ, x, high)
        remote(a, a, n_send.at[2 * r], n_recv.at[2 * r], z_up, t).start()
        remote(b, b, n_send.at[2 * r + 1], n_recv.at[2 * r + 1], z_down, t).start()

    def z_arrived(r):
        low, high = (0, 1) if r == 4 else (None, None)
        arrived(block((z + NZ - r) % NZ, x, low), n_recv.at[2 * r])
        arrived(block((z + r) % NZ, x, high), n_recv.at[2 * r + 1])

    def x_hop(d):
        a = block((z + d) % NZ, x)
        for i, to in enumerate((x_up, x_down, x_far)):
            remote(a, a, m_send.at[3 * d + i], m_recv.at[3 * d + i], z * NX + to, t).start()

    def forward(lo, hi):
        rows = pl.ds(lo * CR, (hi - lo) * CR)
        gu = dot(wgu[...], xd[0, rows, :], 1, 1)
        dh = dot(wd[...], xd[1, rows, :], 1, 1)
        g, u = gu[:FFL], gu[FFL:]
        sig = 1.0 / (1.0 + jnp.exp(-g))
        act = g * sig
        hid_t[:, rows] = (act * u).astype(BF)
        dgu_t[0:FFL, rows] = (dh * u * (sig * (1.0 + g * (1.0 - sig)))).astype(BF)
        dgu_t[FFL : 2 * FFL, rows] = (dh * act).astype(BF)

    def grads(lo, hi):
        def body(i, carry):
            cs = cols(i)
            og_gu[:, cs] = dot(dgu_t[...], xd[0, :, cs], 1, 0).astype(BF)
            og_down[:, cs] = dot(hid_t[...], xd[1, :, cs], 1, 0).astype(BF)
            return carry

        lax.fori_loop(lo, hi, body, 0)

    def dx(m):
        rows = pl.ds(m * PR, PR)
        dg = dgu_t[:, rows].T

        def body(i, carry):
            part[i % 2, i // 2, rows, :] = dot(dg, wgu[:, cols(i)], 1, 0).astype(BF)
            return carry

        lax.fori_loop(0, 8, body, 0)

    def d_rows(m):
        return pl.ds(m * PR, PR)

    def d0(m):
        remote(
            part.at[1 - c, :, d_rows(m), :],
            sib.at[:, d_rows(m), :],
            d_send.at[m * 4],
            d_recv.at[m * 4],
            s,
            t_sib,
        ).start()

    def d1(m):
        arrived(sib.at[:, d_rows(m), :], d_recv.at[m * 4])
        ssum[:, d_rows(m), :] = (
            part[c, :, d_rows(m), :].astype(F32) + sib[:, d_rows(m), :].astype(F32)
        ).astype(BF)
        for i, (to, peer) in enumerate(((far, t_far), (up, t_up), (down, t_down))):
            remote(
                ssum.at[to, d_rows(m), :],
                along.at[i, d_rows(m), :],
                d_send.at[m * 4 + 1 + i],
                d_recv.at[m * 4 + 1 + i],
                s,
                peer,
            ).start()

    def e_copy(k, xx):
        target = ((z + NZ - ORDER[k]) % NZ) * NX + xx
        i = k * NX + xx
        return remote(
            rsum.at[pl.ds(pl.multiple_of(i * CAP, CAP), CAP), :],
            ret.at[pl.ds(pl.multiple_of(s * CAP, CAP), CAP), :],
            e_send.at[i],
            e_recv.at[s],
            target,
            t,
        )

    def d3(m):
        for i in range(3):
            arrived(along.at[i, d_rows(m), :], d_recv.at[m * 4 + 1 + i])
        rsum[d_rows(m), :] = (
            ssum[y, d_rows(m), :].astype(F32)
            + along[0, d_rows(m), :].astype(F32)
            + along[1, d_rows(m), :].astype(F32)
            + along[2, d_rows(m), :].astype(F32)
        ).astype(BF)
        for k in (2 * m, 2 * m + 1):
            each_x(1 if k == 0 else 0, lambda xx: e_copy(k, xx).start())
        if m == 0:
            ret[pl.ds(pl.multiple_of(s * CAP, CAP), CAP), :] = rsum[here, :]

    z_hop(1)
    for k in range(NK):
        a_start(k)
    xd[:, here, cols(t)] = send[:, pl.ds(pl.multiple_of(s * CAP, CAP), CAP), :]
    x_hop(0)
    for k in range(NK):
        a_wait(k)
        chunk[k][0]()
        if k >= 1:
            chunk[k - 1][1]()
        if k >= 2:
            chunk[k - 2][2]()
        if k == 3:
            z_arrived(1)
            z_hop(2)
            x_hop(1)
            x_hop(7)
        if k == 5:
            z_arrived(2)
            z_hop(3)
            x_hop(2)
            x_hop(6)
    for k in range(4):
        chunk[k][3]()
    for load in loads:
        load.wait()
    forward(0, 4)
    chunk[7][1]()
    chunk[6][2]()
    dx(0)
    d0(0)
    chunk[7][2]()
    z_arrived(3)
    z_hop(4)
    x_hop(3)
    x_hop(5)
    dx(1)
    d0(1)
    d1(0)
    chunk[4][3]()
    chunk[5][3]()
    forward(4, 6)
    d1(1)
    dx(2)
    d0(2)
    d3(0)
    chunk[6][3]()
    chunk[7][3]()
    forward(6, 8)
    d1(2)
    dx(3)
    d0(3)
    z_arrived(4)
    x_hop(4)
    d3(1)
    grads(0, 1)
    d1(3)
    d3(2)
    grads(1, 4)
    d3(3)
    grads(4, 8)
    stores = [
        pltpu.make_async_copy(og_gu.at[pl.ds(0, FFL), :], g_gate.at[0], o_sem.at[0]),
        pltpu.make_async_copy(og_gu.at[pl.ds(FFL, FFL), :], g_up.at[0], o_sem.at[1]),
        pltpu.make_async_copy(og_down, g_down.at[0], o_sem.at[2]),
    ]
    for store in stores:
        store.start()
    for load in small[6:]:
        load.wait()

    def e_wait(i, carry):
        e = (s + i) % NSP
        arrived(ret.at[pl.ds(pl.multiple_of(e * CAP, CAP), CAP), :], e_recv.at[e])
        return carry

    lax.fori_loop(1, NSP, e_wait, 0)

    dh = out_grad[...].astype(F32) + dot(place[...], ret[...], 0, 0)
    js[...] = dh.T.astype(BF)
    hf[:, cols(t)] = dh.astype(BF)

    own_cols = pl.ds(pl.multiple_of(s * TOK, TOK), TOK)
    for j in range(NX):
        mine = jnp.logical_and(z == t, x == j)

        @pl.when(jnp.logical_not(mine))
        def _():
            remote(
                js.at[pl.ds(64 * j, 64), :],
                dt.at[:, own_cols],
                j_send.at[j],
                j_recv.at[x],
                t * NX + j,
                z,
            ).start()

        @pl.when(mine)
        def _():
            dt[:, own_cols] = js[pl.ds(64 * j, 64), :]

    def h_piece(tp):
        return hf.at[:, cols(tp)]

    def j_piece(tp):
        return dt.at[:, cols(tp, 512)]

    hg = gather(h_piece, lambda i: h_send.at[i], lambda i: h_recv.at[i])
    jg = gather(j_piece, lambda i: k_send.at[i], lambda i: k_recv.at[i])
    hg[0]()
    hg[1]()
    for j in range(NX):

        @pl.when(jnp.logical_not(jnp.logical_and(z == t, x == j)))
        def _():
            arrived(
                dt.at[:, pl.ds(pl.multiple_of(t * 512 + j * TOK, TOK), TOK)], j_recv.at[j]
            )

    jg[0]()
    hg[2]()
    dz = dot(hf[...], out_proj[...], 1, 0)
    dconv = (dz * gate_b[...].astype(F32)).astype(BF)
    hsend[...] = dconv

    @pl.when(s < NSP - 1)
    def _():
        remote(
            hsend.at[pl.ds(TOK - 16, 16), :], halo.at[0], j_send.at[4], j_recv.at[4], s + 1, t
        ).start()

    @pl.when(s > 0)
    def _():
        remote(hsend.at[pl.ds(0, 16), :], halo.at[1], j_send.at[5], j_recv.at[5], s - 1, t).start()

    jg[1]()
    g_b[...] = (dz * conv_out[...].astype(F32)).astype(BF)

    @pl.when(s > 0)
    def _():
        arrived(halo.at[0], j_recv.at[4])

    @pl.when(s == 0)
    def _():
        halo[0] = jnp.zeros((16, CH), BF)

    @pl.when(s < NSP - 1)
    def _():
        arrived(halo.at[1], j_recv.at[5])

    @pl.when(s == NSP - 1)
    def _():
        halo[1] = jnp.zeros((16, CH), BF)

    d = dconv.astype(F32)
    at_row = lax.broadcasted_iota(jnp.int32, (TOK, CH), 0)
    before_first = halo[0].astype(F32)[15:16, :]
    after_last = halo[1].astype(F32)[0:1, :]
    earlier_rows = jnp.where(at_row == 0, before_first, pltpu.roll(d, 1, 0))
    later_rows = jnp.where(at_row == TOK - 1, after_last, pltpu.roll(d, TOK - 1, 0))
    tp3 = taps[...]
    grad_u = tp3[0:1, :] * later_rows + tp3[1:2, :] * d + tp3[2:3, :] * earlier_rows
    g_c[...] = (grad_u * value_v[...].astype(F32)).astype(BF)
    g_v[...] = (grad_u * gate_c[...].astype(F32)).astype(BF)

    for d in range(NZ):
        for i, source in enumerate((x_down, x_up, x_far)):
            arrived(block((z + d) % NZ, source), m_recv.at[3 * d + i])
    jg[2]()
    g_out[...] = dot(dt[...], mx[...], 1, 0)
    late = [
        pltpu.make_async_copy(a, b, o_sem.at[3 + i])
        for i, (a, b) in enumerate(((g_out, g_out_h), (g_b, g_b_h), (g_c, g_c_h), (g_v, g_v_h)))
    ]
    for store in late:
        store.start()
    stores += late

    for k in range(NK):
        each_x(1 if k == 0 else 0, lambda xx: a_copy(k, xx).wait_send())
        each_x(1 if k == 0 else 0, lambda xx: e_copy(k, xx).wait_send())
        chunk[k][4]()
    for m in range(NP):
        left(part.at[0, :, d_rows(m), :], d_send.at[m * 4])
        for i in range(3):
            left(along.at[i, d_rows(m), :], d_send.at[m * 4 + 1 + i])
    hg[3]()
    jg[3]()
    for d in range(NZ):
        for i in range(3):
            left(block(z, x), m_send.at[3 * d + i])
    for r in range(1, 5):
        half = 0 if r == 4 else None
        left(block(z, x, half), n_send.at[2 * r])
        left(block(z, x, half), n_send.at[2 * r + 1])
    for j in range(NX):

        @pl.when(jnp.logical_not(jnp.logical_and(z == t, x == j)))
        def _():
            left(js.at[pl.ds(64 * j, 64), :], j_send.at[j])

    @pl.when(s < NSP - 1)
    def _():
        left(halo.at[0], j_send.at[4])

    @pl.when(s > 0)
    def _():
        left(halo.at[1], j_send.at[5])

    for store in stores:
        store.wait()


def emit(*refs):
    ins, outs, held = refs[:7], refs[7:14], refs[14:21]
    i_sem, o_sem = refs[21:]
    pieces = []
    for a, b, v in zip(ins, outs, held):
        if len(a.shape) == 3:
            half = a.shape[1] // 2
            pieces += [tuple(r.at[:, pl.ds(i * half, half), :] for r in (a, b, v)) for i in range(2)]
        else:
            pieces.append((a, b, v))
    loads = [pltpu.make_async_copy(a, v, i_sem.at[i]) for i, (a, _, v) in enumerate(pieces)]
    stores = [pltpu.make_async_copy(v, b, o_sem.at[i]) for i, (_, b, v) in enumerate(pieces)]
    for load in loads:
        load.start()
    for load, store in zip(loads, stores):
        load.wait()
        store.start()
    for store in stores:
        store.wait()


def local(
    out_grad,
    moe_input,
    route_weight,
    route_ids,
    gate_proj,
    up_proj,
    down_proj,
    out_proj,
    conv_out,
    gate_b,
    gate_c,
    value_v,
    conv_taps,
):
    hbm = pl.BlockSpec(memory_space=pl.ANY)
    dma = pltpu.SemaphoreType.DMA
    shape = jax.ShapeDtypeStruct
    kept = pl.pallas_call(
        kernel,
        out_shape=(
            shape((1, FFL, D), BF),
            shape((1, FFL, D), BF),
            shape((1, FFL, D), BF),
            shape((64, CH), F32),
            shape((TOK, CH), BF),
            shape((TOK, CH), BF),
            shape((TOK, CH), BF),
        ),
        in_specs=[hbm] * 13,
        out_specs=(hbm,) * 7,
        scratch_shapes=[
            pltpu.VMEM((TOK, CH), BF),
            pltpu.VMEM((TOK, CH), BF),
            pltpu.VMEM((2, TOK), F32),
            pltpu.VMEM((2, TOK), jnp.int32),
            pltpu.VMEM((D, CH), BF),
            pltpu.VMEM((TOK, CH), BF),
            pltpu.VMEM((TOK, CH), BF),
            pltpu.VMEM((TOK, CH), BF),
            pltpu.VMEM((TOK, CH), BF),
            pltpu.VMEM((3, CH), F32),
            pltpu.VMEM((64, CH), F32),
            pltpu.VMEM((TOK, CH), BF),
            pltpu.VMEM((TOK, CH), BF),
            pltpu.VMEM((TOK, CH), BF),
            pltpu.VMEM((2 * FFL, D), BF),
            pltpu.VMEM((FFL, D), BF),
            dma((10,)),
            dma((7,)),
            pltpu.VMEM((2, ROWS, CH), BF),
            pltpu.VMEM((2, ROWS, D), BF),
            pltpu.VMEM((2 * FFL, D), BF),
            pltpu.VMEM((FFL, D), BF),
            pltpu.VMEM((ROWS, TOK), BF),
            pltpu.VMEM((2 * FFL, ROWS), BF),
            pltpu.VMEM((FFL, ROWS), BF),
            pltpu.VMEM((2, NY, ROWS, CH), BF),
            pltpu.VMEM((NY, ROWS, CH), BF),
            pltpu.VMEM((NY, ROWS, CH), BF),
            pltpu.VMEM((3, ROWS, CH), BF),
            pltpu.VMEM((ROWS, CH), BF),
            pltpu.VMEM((ROWS, CH), BF),
            pltpu.VMEM((TOK, D), BF),
            pltpu.VMEM((CH, TOK), BF),
            pltpu.VMEM((64, NSP * TOK), BF),
            pltpu.VMEM((NSP * TOK, CH), BF),
            pltpu.VMEM((TOK, CH), BF),
            pltpu.VMEM((2, 16, CH), BF),
            dma((3,)),
            dma((NSP,)),
            dma((NSP,)),
            dma((9 * NK,)),
            dma((9 * NK,)),
            dma((4 * NP,)),
            dma((4 * NP,)),
            dma((NSP,)),
            dma((NSP,)),
            dma((7,)),
            dma((7,)),
            dma((6,)),
            dma((6,)),
            dma((7,)),
            dma((7,)),
            dma((3 * NZ,)),
            dma((3 * NZ,)),
            dma((10,)),
            dma((10,)),
        ],
        compiler_params=pltpu.CompilerParams(
            collective_id=0, has_side_effects=True, vmem_limit_bytes=60 * 1024 * 1024
        ),
        name="layer",
    )(
        out_grad,
        moe_input,
        route_weight.T,
        route_ids.T,
        gate_proj.transpose(0, 2, 1),
        up_proj.transpose(0, 2, 1),
        down_proj,
        out_proj,
        conv_out,
        gate_b,
        gate_c,
        value_v,
        conv_taps,
    )
    g_gate, g_up, g_down, g_out, g_b, g_c, g_v = pl.pallas_call(
        emit,
        out_shape=tuple(shape(a.shape, a.dtype) for a in kept),
        in_specs=[hbm] * 7,
        out_specs=(hbm,) * 7,
        scratch_shapes=[pltpu.VMEM(a.shape, a.dtype) for a in kept] + [dma((10,)), dma((10,))],
        compiler_params=pltpu.CompilerParams(vmem_limit_bytes=60 * 1024 * 1024),
        name="emit",
    )(*kept)
    return g_gate.transpose(0, 2, 1), g_up.transpose(0, 2, 1), g_down, g_out, g_b, g_c, g_v


def solution(mesh):
    return jax.shard_map(
        local,
        mesh=mesh,
        in_specs=(
            P("sp", "tp"),
            P("sp", "tp"),
            P("sp", None),
            P("sp", None),
            P("sp", None, "tp"),
            P("sp", None, "tp"),
            P("sp", "tp", None),
            P(None, "tp"),
            P("sp", "tp"),
            P("sp", "tp"),
            P("sp", "tp"),
            P("sp", "tp"),
            P(None, "tp"),
        ),
        out_specs=(
            P("sp", None, "tp"),
            P("sp", None, "tp"),
            P("sp", "tp", None),
            P("sp", "tp"),
            P("sp", "tp"),
            P("sp", "tp"),
            P("sp", "tp"),
        ),
        check_vma=False,
    )
```

```python
import jax
import jax.numpy as jnp
from jax import lax
from jax.experimental import pallas as pl
from jax.experimental.pallas import tpu as pltpu
from jax.sharding import PartitionSpec as P

MESH = pl.DeviceIdType.MESH
BF = jnp.bfloat16
F32 = jnp.float32
NZ, NX, NY = 8, 4, 4
NSP = NZ * NX
CAP = 16
TOK = 128
CH = 256
D = 2048
FFL = 352
ROWS = NSP * CAP
NK = 8
CR = ROWS // NK
NP = 4
PR = ROWS // NP
ORDER = (0, 1, 7, 3, 5, 4, 2, 6)


def dot(a, b, ca, cb):
    return lax.dot_general(a, b, (((ca,), (cb,)), ((), ())), preferred_element_type=F32)


def kernel(
    out_grad_h,
    moe_input_h,
    weight_h,
    ids_h,
    gate_proj,
    up_proj,
    down_proj,
    out_proj_h,
    conv_out_h,
    gate_b_h,
    gate_c_h,
    value_v_h,
    taps_h,
    g_gate,
    g_up,
    g_down,
    g_out_h,
    g_b_h,
    g_c_h,
    g_v_h,
    out_grad,
    moe_input,
    weight_t,
    ids_t,
    out_proj,
    conv_out,
    gate_b,
    gate_c,
    value_v,
    taps,
    g_out,
    g_b,
    g_c,
    g_v,
    og_gu,
    og_down,
    i_sem,
    o_sem,
    send,
    xd,
    wgu,
    wd,
    place,
    dgu_t,
    hid_t,
    part,
    sib,
    ssum,
    along,
    rsum,
    ret,
    hf,
    js,
    dt,
    mx,
    hsend,
    halo,
    w_sem,
    a_send,
    a_recv,
    b_send,
    b_recv,
    d_send,
    d_recv,
    e_send,
    e_recv,
    h_send,
    h_recv,
    j_send,
    j_recv,
    k_send,
    k_recv,
    m_send,
    m_recv,
    n_send,
    n_recv,
):
    s = lax.axis_index("sp")
    t = lax.axis_index("tp")
    z, x = s // NX, s % NX
    y, c = t // 2, t % 2
    up, down, far = (y + 1) % NY, (y + NY - 1) % NY, (y + 2) % NY
    t_up, t_down, t_sib = up * 2 + c, down * 2 + c, y * 2 + (1 - c)
    t_far = far * 2 + c

    def remote(src, dst, ssem, rsem, sp, tp):
        return pltpu.make_async_remote_copy(
            src_ref=src,
            dst_ref=dst,
            send_sem=ssem,
            recv_sem=rsem,
            device_id={"sp": sp, "tp": tp},
            device_id_type=MESH,
        )

    def arrived(ref, rsem):
        remote(ref, ref, n_send.at[0], rsem, s, t).wait_recv()

    def left(ref, ssem):
        remote(ref, ref, ssem, n_recv.at[0], s, t).wait_send()

    barrier = pltpu.get_barrier_semaphore()

    def greet(i, carry):
        pl.semaphore_signal(
            barrier, inc=1, device_id={"sp": (s + i) % NSP, "tp": t}, device_id_type=MESH
        )
        return carry

    lax.fori_loop(1, NSP, greet, 0)
    for peer in (t_up, t_down, t_far, t_sib):
        pl.semaphore_signal(barrier, inc=1, device_id={"sp": s, "tp": peer}, device_id_type=MESH)
    cross = (z + NZ // 2) % NZ
    back = (t + NZ // 2) % NZ
    for j in range(NX):
        pl.semaphore_signal(
            barrier, inc=1, device_id={"sp": t * NX + j, "tp": cross}, device_id_type=MESH
        )
        pl.semaphore_signal(
            barrier, inc=1, device_id={"sp": back * NX + j, "tp": z}, device_id_type=MESH
        )

    small = [
        pltpu.make_async_copy(a, b, i_sem.at[i])
        for i, (a, b) in enumerate(
            (
                (ids_h, ids_t),
                (weight_h, weight_t),
                (out_grad_h, out_grad),
                (moe_input_h, moe_input),
                (gate_b_h, gate_b),
                (conv_out_h, conv_out),
                (gate_c_h, gate_c),
                (value_v_h, value_v),
                (taps_h, taps),
                (out_proj_h, out_proj),
            )
        )
    ]
    loads = [
        pltpu.make_async_copy(gate_proj.at[0], wgu.at[pl.ds(0, FFL), :], w_sem.at[0]),
        pltpu.make_async_copy(up_proj.at[0], wgu.at[pl.ds(FFL, FFL), :], w_sem.at[1]),
        pltpu.make_async_copy(down_proj.at[0], wd, w_sem.at[2]),
    ]
    for load in small:
        load.start()
    for load in loads:
        load.start()

    for load in small[:6]:
        load.wait()

    ids = ids_t[...]
    experts = lax.broadcasted_iota(jnp.int32, (NSP, TOK), 0)
    e0 = jnp.where(experts == ids[0:1, :], 1.0, 0.0).astype(F32)
    e1 = jnp.where(experts == ids[1:2, :], 1.0, 0.0).astype(F32)
    row = lax.broadcasted_iota(jnp.int32, (TOK, TOK), 0)
    col = lax.broadcasted_iota(jnp.int32, (TOK, TOK), 1)
    earlier = jnp.where(row < col, 1.0, 0.0).astype(BF)
    before = dot((e0 + e1).astype(BF), earlier, 1, 0)
    slot0 = jnp.sum(before * e0, axis=0, keepdims=True)
    slot1 = jnp.sum(before * e1, axis=0, keepdims=True)
    idf = ids.astype(F32) * CAP
    at = lax.broadcasted_iota(jnp.int32, (ROWS, TOK), 0).astype(F32)
    p0 = jnp.where(at == idf[0:1, :] + slot0, 1.0, 0.0).astype(BF)
    p1 = jnp.where(at == idf[1:2, :] + slot1, 1.0, 0.0).astype(BF)
    place[...] = p0 + p1
    og = out_grad[...].astype(F32)
    w = weight_t[...]
    w0 = jnp.broadcast_to(w[0:1, :], (TOK, TOK)).T
    w1 = jnp.broadcast_to(w[1:2, :], (TOK, TOK)).T
    dy0 = (jnp.concatenate([w0, w0], axis=1) * og).astype(BF)
    dy1 = (jnp.concatenate([w1, w1], axis=1) * og).astype(BF)
    send[0] = dot(p0 + p1, moe_input[...], 1, 0).astype(BF)
    send[1] = (dot(p0, dy0, 1, 0) + dot(p1, dy1, 1, 0)).astype(BF)
    mixed = (gate_b[...].astype(F32) * conv_out[...].astype(F32)).astype(BF)
    own_rows = pl.ds(pl.multiple_of((x * NZ + z) * TOK, TOK), TOK)
    mx[own_rows, :] = mixed

    def cols(tp, width=CH):
        return pl.ds(pl.multiple_of(tp * width, width), width)

    pl.semaphore_wait(barrier, NSP - 1 + 4 + 8)

    def a_copy(k, xx):
        target = ((z + ORDER[k]) % NZ) * NX + xx
        src = send.at[:, pl.ds(pl.multiple_of(target * CAP, CAP), CAP), :]
        dst = xd.at[:, pl.ds(pl.multiple_of(k * CR + x * CAP, CAP), CAP), cols(t)]
        return remote(src, dst, a_send.at[k * NX + xx], a_recv.at[k * NX + x], target, t)

    def each_x(first, do):
        def body(i, carry):
            do((x + i) % NX)
            return carry

        lax.fori_loop(first, NX, body, 0)

    def a_start(k):
        each_x(1 if k == 0 else 0, lambda xx: a_copy(k, xx).start())

    def a_wait(k):
        def one(xx):
            arrived(
                xd.at[:, pl.ds(pl.multiple_of(k * CR + xx * CAP, CAP), CAP), cols(t)],
                a_recv.at[k * NX + xx],
            )

        each_x(1 if k == 0 else 0, one)

    here = pl.ds(pl.multiple_of(x * CAP, CAP), CAP)

    def gather(piece, ss, rs):
        def one():
            for i, peer in enumerate((t_sib, t_up, t_down, t_far)):
                remote(piece(t), piece(t), ss(i), rs(i), s, peer).start()

        def two():
            for i, origin in enumerate((t_down, t_up, t_far)):
                arrived(piece(origin), rs(1 + i))
                remote(piece(origin), piece(origin), ss(4 + i), rs(4 + i), s, t_sib).start()

        def three():
            for i, origin in enumerate((y, down, up, far)):
                arrived(piece(origin * 2 + 1 - c), rs(i if i == 0 else 3 + i))

        def end():
            for i in range(7):
                left(piece(t), ss(i))

        return one, two, three, end

    def relay(piece, ss, rs):
        def one():
            for i, peer in enumerate((t_sib, t_up, t_down)):
                remote(piece(t), piece(t), ss(i), rs(i), s, peer).start()

        def two():
            for i, (origin, peer) in enumerate(((t_down, t_up), (t_up, t_down))):
                arrived(piece(origin), rs(1 + i))
                half = piece(origin, i)
                remote(half, half, ss(3 + i), rs(3 + i), s, peer).start()
                remote(piece(origin), piece(origin), ss(5 + i), rs(5 + i), s, t_sib).start()

        def three():
            for i in range(2):
                half = piece(t_far, i)
                arrived(half, rs(3 + i))
                remote(half, half, ss(7 + i), rs(7 + i), s, t_sib).start()

        def four():
            arrived(piece(t_sib), rs(0))
            arrived(piece(down * 2 + 1 - c), rs(5))
            arrived(piece(up * 2 + 1 - c), rs(6))
            arrived(piece(far * 2 + 1 - c, 0), rs(7))
            arrived(piece(far * 2 + 1 - c, 1), rs(8))

        def end():
            for i in range(9):
                left(piece(t) if i in (0, 1, 2, 5, 6) else piece(t, 0), ss(i))

        return one, two, three, four, end

    def chunk_piece(k):
        rows = pl.ds(k * CR, CR)

        def piece(tp, half=None):
            if half is None:
                return xd.at[:, rows, cols(tp)]
            return xd.at[half, rows, cols(tp)]

        return piece

    chunk = [
        relay(
            chunk_piece(k),
            lambda i, k=k: b_send.at[k * 9 + i],
            lambda i, k=k: b_recv.at[k * 9 + i],
        )
        for k in range(NK)
    ]

    def block(zz, xx, half=None):
        base = (xx * NZ + zz) * TOK
        if half is None:
            return mx.at[pl.ds(pl.multiple_of(base, TOK), TOK), :]
        return mx.at[pl.ds(pl.multiple_of(base + half * (TOK // 2), TOK // 2), TOK // 2), :]

    z_up, z_down = ((z + 1) % NZ) * NX + x, ((z + NZ - 1) % NZ) * NX + x
    x_up, x_down, x_far = (x + 1) % NX, (x + NX - 1) % NX, (x + 2) % NX

    def z_hop(r):
        low, high = (0, 1) if r == 4 else (None, None)
        a = block((z + NZ - (r - 1)) % NZ, x, low)
        b = block((z + r - 1) % NZ, x, high)
        remote(a, a, n_send.at[2 * r], n_recv.at[2 * r], z_up, t).start()
        remote(b, b, n_send.at[2 * r + 1], n_recv.at[2 * r + 1], z_down, t).start()

    def z_arrived(r):
        low, high = (0, 1) if r == 4 else (None, None)
        arrived(block((z + NZ - r) % NZ, x, low), n_recv.at[2 * r])
        arrived(block((z + r) % NZ, x, high), n_recv.at[2 * r + 1])

    def x_hop(d):
        a = block((z + d) % NZ, x)
        for i, to in enumerate((x_up, x_down, x_far)):
            remote(a, a, m_send.at[3 * d + i], m_recv.at[3 * d + i], z * NX + to, t).start()

    def forward(lo, hi):
        rows = pl.ds(lo * CR, (hi - lo) * CR)
        gu = dot(wgu[...], xd[0, rows, :], 1, 1)
        dh = dot(wd[...], xd[1, rows, :], 1, 1)
        g, u = gu[:FFL], gu[FFL:]
        sig = 1.0 / (1.0 + jnp.exp(-g))
        act = g * sig
        hid_t[:, rows] = (act * u).astype(BF)
        dgu_t[0:FFL, rows] = (dh * u * (sig * (1.0 + g * (1.0 - sig)))).astype(BF)
        dgu_t[FFL : 2 * FFL, rows] = (dh * act).astype(BF)

    def grads(lo, hi):
        def body(i, carry):
            cs = cols(i)
            og_gu[:, cs] = dot(dgu_t[...], xd[0, :, cs], 1, 0).astype(BF)
            og_down[:, cs] = dot(hid_t[...], xd[1, :, cs], 1, 0).astype(BF)
            return carry

        lax.fori_loop(lo, hi, body, 0)

    def dx(m):
        rows = pl.ds(m * PR, PR)
        dg = dgu_t[:, rows].T

        def body(i, carry):
            part[i % 2, i // 2, rows, :] = dot(dg, wgu[:, cols(i)], 1, 0).astype(BF)
            return carry

        lax.fori_loop(0, 8, body, 0)

    def d_rows(m):
        return pl.ds(m * PR, PR)

    def d0(m):
        remote(
            part.at[1 - c, :, d_rows(m), :],
            sib.at[:, d_rows(m), :],
            d_send.at[m * 4],
            d_recv.at[m * 4],
            s,
            t_sib,
        ).start()

    def d1(m):
        arrived(sib.at[:, d_rows(m), :], d_recv.at[m * 4])
        ssum[:, d_rows(m), :] = (
            part[c, :, d_rows(m), :].astype(F32) + sib[:, d_rows(m), :].astype(F32)
        ).astype(BF)
        for i, (to, peer) in enumerate(((far, t_far), (up, t_up), (down, t_down))):
            remote(
                ssum.at[to, d_rows(m), :],
                along.at[i, d_rows(m), :],
                d_send.at[m * 4 + 1 + i],
                d_recv.at[m * 4 + 1 + i],
                s,
                peer,
            ).start()

    def e_copy(k, xx):
        target = ((z + NZ - ORDER[k]) % NZ) * NX + xx
        i = k * NX + xx
        return remote(
            rsum.at[pl.ds(pl.multiple_of(i * CAP, CAP), CAP), :],
            ret.at[pl.ds(pl.multiple_of(s * CAP, CAP), CAP), :],
            e_send.at[i],
            e_recv.at[s],
            target,
            t,
        )

    def d3(m):
        for i in range(3):
            arrived(along.at[i, d_rows(m), :], d_recv.at[m * 4 + 1 + i])
        rsum[d_rows(m), :] = (
            ssum[y, d_rows(m), :].astype(F32)
            + along[0, d_rows(m), :].astype(F32)
            + along[1, d_rows(m), :].astype(F32)
            + along[2, d_rows(m), :].astype(F32)
        ).astype(BF)
        for k in (2 * m, 2 * m + 1):
            each_x(1 if k == 0 else 0, lambda xx: e_copy(k, xx).start())
        if m == 0:
            ret[pl.ds(pl.multiple_of(s * CAP, CAP), CAP), :] = rsum[here, :]

    z_hop(1)
    for k in range(NK):
        a_start(k)
    xd[:, here, cols(t)] = send[:, pl.ds(pl.multiple_of(s * CAP, CAP), CAP), :]
    x_hop(0)
    for k in range(NK):
        a_wait(k)
        chunk[k][0]()
        if k >= 2:
            chunk[k - 2][1]()
        if k >= 4:
            chunk[k - 4][2]()
        if k == 4:
            z_arrived(1)
            z_hop(2)
            x_hop(1)
            x_hop(7)
        if k == 6:
            z_arrived(2)
            z_hop(3)
            x_hop(2)
            x_hop(6)
    chunk[6][1]()
    chunk[4][2]()
    for load in loads:
        load.wait()
    chunk[0][3]()
    chunk[1][3]()
    chunk[2][3]()
    chunk[3][3]()
    forward(0, 4)
    chunk[7][1]()
    chunk[5][2]()
    dx(0)
    d0(0)
    chunk[6][2]()
    dx(1)
    d0(1)
    d1(0)
    z_arrived(3)
    z_hop(4)
    x_hop(3)
    x_hop(5)
    chunk[7][2]()
    chunk[4][3]()
    chunk[5][3]()
    forward(4, 6)
    d1(1)
    dx(2)
    d0(2)
    chunk[6][3]()
    chunk[7][3]()
    forward(6, 8)
    d1(2)
    dx(3)
    d0(3)
    d3(0)
    z_arrived(4)
    x_hop(4)
    d3(1)
    d1(3)
    grads(0, 2)
    d3(2)
    grads(2, 4)
    d3(3)
    grads(4, 8)
    stores = [
        pltpu.make_async_copy(og_gu.at[pl.ds(0, FFL), :], g_gate.at[0], o_sem.at[0]),
        pltpu.make_async_copy(og_gu.at[pl.ds(FFL, FFL), :], g_up.at[0], o_sem.at[1]),
        pltpu.make_async_copy(og_down, g_down.at[0], o_sem.at[2]),
    ]
    for store in stores:
        store.start()
    for load in small[6:]:
        load.wait()

    def e_wait(i, carry):
        e = (s + i) % NSP
        arrived(ret.at[pl.ds(pl.multiple_of(e * CAP, CAP), CAP), :], e_recv.at[e])
        return carry

    lax.fori_loop(1, NSP, e_wait, 0)

    dh = out_grad[...].astype(F32) + dot(place[...], ret[...], 0, 0)
    js[...] = dh.T.astype(BF)
    hf[:, cols(t)] = dh.astype(BF)

    def token_cols(zz, xx):
        return pl.ds(pl.multiple_of((xx * NZ + zz) * TOK, TOK), TOK)

    for j in range(NX):
        remote(
            js.at[pl.ds(64 * j, 64), :],
            dt.at[:, token_cols(z, x)],
            j_send.at[j],
            j_recv.at[x],
            t * NX + j,
            cross,
        ).start()

    def h_piece(tp):
        return hf.at[:, cols(tp)]

    x_order = (x, (x + 1) % NX, (x + NX - 1) % NX, (x + 2) % NX)

    def j_piece(i):
        return lambda tp: dt.at[:, token_cols((tp + NZ // 2) % NZ, x_order[i])]

    hg = gather(h_piece, lambda i: h_send.at[i], lambda i: h_recv.at[i])
    jg = [
        gather(
            j_piece(i),
            lambda n, i=i: k_send.at[7 * i + n],
            lambda n, i=i: k_recv.at[7 * i + n],
        )
        for i in range(NX)
    ]
    hg[0]()
    hg[1]()
    for i in range(NX):
        arrived(dt.at[:, token_cols(back, x_order[i])], j_recv.at[x_order[i]])
        jg[i][0]()
    hg[2]()
    dz = dot(hf[...], out_proj[...], 1, 0)
    dconv = (dz * gate_b[...].astype(F32)).astype(BF)
    hsend[...] = dconv

    @pl.when(s < NSP - 1)
    def _():
        remote(
            hsend.at[pl.ds(TOK - 16, 16), :], halo.at[0], j_send.at[4], j_recv.at[4], s + 1, t
        ).start()

    @pl.when(s > 0)
    def _():
        remote(hsend.at[pl.ds(0, 16), :], halo.at[1], j_send.at[5], j_recv.at[5], s - 1, t).start()

    for i in range(NX):
        jg[i][1]()
    g_b[...] = (dz * conv_out[...].astype(F32)).astype(BF)

    @pl.when(s > 0)
    def _():
        arrived(halo.at[0], j_recv.at[4])

    @pl.when(s == 0)
    def _():
        halo[0] = jnp.zeros((16, CH), BF)

    @pl.when(s < NSP - 1)
    def _():
        arrived(halo.at[1], j_recv.at[5])

    @pl.when(s == NSP - 1)
    def _():
        halo[1] = jnp.zeros((16, CH), BF)

    d = dconv.astype(F32)
    at_row = lax.broadcasted_iota(jnp.int32, (TOK, CH), 0)
    before_first = halo[0].astype(F32)[15:16, :]
    after_last = halo[1].astype(F32)[0:1, :]
    earlier_rows = jnp.where(at_row == 0, before_first, pltpu.roll(d, 1, 0))
    later_rows = jnp.where(at_row == TOK - 1, after_last, pltpu.roll(d, TOK - 1, 0))
    tp3 = taps[...]
    grad_u = tp3[0:1, :] * later_rows + tp3[1:2, :] * d + tp3[2:3, :] * earlier_rows
    g_c[...] = (grad_u * value_v[...].astype(F32)).astype(BF)
    g_v[...] = (grad_u * gate_c[...].astype(F32)).astype(BF)

    for d in range(NZ):
        for i, source in enumerate((x_down, x_up, x_far)):
            arrived(block((z + d) % NZ, source), m_recv.at[3 * d + i])
    total = jnp.zeros((64, CH), F32)
    for i in range(NX):
        jg[i][2]()
        ks = pl.ds(pl.multiple_of(x_order[i] * (NZ * TOK), NZ * TOK), NZ * TOK)
        total += dot(dt[:, ks], mx[ks, :], 1, 0)
    g_out[...] = total
    late = [
        pltpu.make_async_copy(a, b, o_sem.at[3 + i])
        for i, (a, b) in enumerate(((g_out, g_out_h), (g_b, g_b_h), (g_c, g_c_h), (g_v, g_v_h)))
    ]
    for store in late:
        store.start()
    stores += late

    for k in range(NK):
        each_x(1 if k == 0 else 0, lambda xx: a_copy(k, xx).wait_send())
        each_x(1 if k == 0 else 0, lambda xx: e_copy(k, xx).wait_send())
        chunk[k][4]()
    for m in range(NP):
        left(part.at[0, :, d_rows(m), :], d_send.at[m * 4])
        for i in range(3):
            left(along.at[i, d_rows(m), :], d_send.at[m * 4 + 1 + i])
    hg[3]()
    for i in range(NX):
        jg[i][3]()
    for d in range(NZ):
        for i in range(3):
            left(block(z, x), m_send.at[3 * d + i])
    for r in range(1, 5):
        half = 0 if r == 4 else None
        left(block(z, x, half), n_send.at[2 * r])
        left(block(z, x, half), n_send.at[2 * r + 1])
    for j in range(NX):
        left(js.at[pl.ds(64 * j, 64), :], j_send.at[j])

    @pl.when(s < NSP - 1)
    def _():
        left(halo.at[0], j_send.at[4])

    @pl.when(s > 0)
    def _():
        left(halo.at[1], j_send.at[5])

    for store in stores:
        store.wait()


def emit(*refs):
    ins, outs, held = refs[:7], refs[7:14], refs[14:21]
    i_sem, o_sem = refs[21:]
    pieces = []
    for a, b, v in zip(ins, outs, held):
        if len(a.shape) == 3:
            half = a.shape[1] // 2
            pieces += [tuple(r.at[:, pl.ds(i * half, half), :] for r in (a, b, v)) for i in range(2)]
        else:
            pieces.append((a, b, v))
    loads = [pltpu.make_async_copy(a, v, i_sem.at[i]) for i, (a, _, v) in enumerate(pieces)]
    stores = [pltpu.make_async_copy(v, b, o_sem.at[i]) for i, (_, b, v) in enumerate(pieces)]
    for load in loads:
        load.start()
    for load, store in zip(loads, stores):
        load.wait()
        store.start()
    for store in stores:
        store.wait()


def local(
    out_grad,
    moe_input,
    route_weight,
    route_ids,
    gate_proj,
    up_proj,
    down_proj,
    out_proj,
    conv_out,
    gate_b,
    gate_c,
    value_v,
    conv_taps,
):
    hbm = pl.BlockSpec(memory_space=pl.ANY)
    dma = pltpu.SemaphoreType.DMA
    shape = jax.ShapeDtypeStruct
    kept = pl.pallas_call(
        kernel,
        out_shape=(
            shape((1, FFL, D), BF),
            shape((1, FFL, D), BF),
            shape((1, FFL, D), BF),
            shape((64, CH), F32),
            shape((TOK, CH), BF),
            shape((TOK, CH), BF),
            shape((TOK, CH), BF),
        ),
        in_specs=[hbm] * 13,
        out_specs=(hbm,) * 7,
        scratch_shapes=[
            pltpu.VMEM((TOK, CH), BF),
            pltpu.VMEM((TOK, CH), BF),
            pltpu.VMEM((2, TOK), F32),
            pltpu.VMEM((2, TOK), jnp.int32),
            pltpu.VMEM((D, CH), BF),
            pltpu.VMEM((TOK, CH), BF),
            pltpu.VMEM((TOK, CH), BF),
            pltpu.VMEM((TOK, CH), BF),
            pltpu.VMEM((TOK, CH), BF),
            pltpu.VMEM((3, CH), F32),
            pltpu.VMEM((64, CH), F32),
            pltpu.VMEM((TOK, CH), BF),
            pltpu.VMEM((TOK, CH), BF),
            pltpu.VMEM((TOK, CH), BF),
            pltpu.VMEM((2 * FFL, D), BF),
            pltpu.VMEM((FFL, D), BF),
            dma((10,)),
            dma((7,)),
            pltpu.VMEM((2, ROWS, CH), BF),
            pltpu.VMEM((2, ROWS, D), BF),
            pltpu.VMEM((2 * FFL, D), BF),
            pltpu.VMEM((FFL, D), BF),
            pltpu.VMEM((ROWS, TOK), BF),
            pltpu.VMEM((2 * FFL, ROWS), BF),
            pltpu.VMEM((FFL, ROWS), BF),
            pltpu.VMEM((2, NY, ROWS, CH), BF),
            pltpu.VMEM((NY, ROWS, CH), BF),
            pltpu.VMEM((NY, ROWS, CH), BF),
            pltpu.VMEM((3, ROWS, CH), BF),
            pltpu.VMEM((ROWS, CH), BF),
            pltpu.VMEM((ROWS, CH), BF),
            pltpu.VMEM((TOK, D), BF),
            pltpu.VMEM((CH, TOK), BF),
            pltpu.VMEM((64, NSP * TOK), BF),
            pltpu.VMEM((NSP * TOK, CH), BF),
            pltpu.VMEM((TOK, CH), BF),
            pltpu.VMEM((2, 16, CH), BF),
            dma((3,)),
            dma((NSP,)),
            dma((NSP,)),
            dma((9 * NK,)),
            dma((9 * NK,)),
            dma((4 * NP,)),
            dma((4 * NP,)),
            dma((NSP,)),
            dma((NSP,)),
            dma((7,)),
            dma((7,)),
            dma((6,)),
            dma((6,)),
            dma((7 * NX,)),
            dma((7 * NX,)),
            dma((3 * NZ,)),
            dma((3 * NZ,)),
            dma((10,)),
            dma((10,)),
        ],
        compiler_params=pltpu.CompilerParams(
            collective_id=0, has_side_effects=True, vmem_limit_bytes=60 * 1024 * 1024
        ),
        name="layer",
    )(
        out_grad,
        moe_input,
        route_weight.T,
        route_ids.T,
        gate_proj.transpose(0, 2, 1),
        up_proj.transpose(0, 2, 1),
        down_proj,
        out_proj,
        conv_out,
        gate_b,
        gate_c,
        value_v,
        conv_taps,
    )
    g_gate, g_up, g_down, g_out, g_b, g_c, g_v = pl.pallas_call(
        emit,
        out_shape=tuple(shape(a.shape, a.dtype) for a in kept),
        in_specs=[hbm] * 7,
        out_specs=(hbm,) * 7,
        scratch_shapes=[pltpu.VMEM(a.shape, a.dtype) for a in kept] + [dma((10,)), dma((10,))],
        compiler_params=pltpu.CompilerParams(vmem_limit_bytes=60 * 1024 * 1024),
        name="emit",
    )(*kept)
    return g_gate.transpose(0, 2, 1), g_up.transpose(0, 2, 1), g_down, g_out, g_b, g_c, g_v


def solution(mesh):
    return jax.shard_map(
        local,
        mesh=mesh,
        in_specs=(
            P("sp", "tp"),
            P("sp", "tp"),
            P("sp", None),
            P("sp", None),
            P("sp", None, "tp"),
            P("sp", None, "tp"),
            P("sp", "tp", None),
            P(None, "tp"),
            P("sp", "tp"),
            P("sp", "tp"),
            P("sp", "tp"),
            P("sp", "tp"),
            P(None, "tp"),
        ),
        out_specs=(
            P("sp", None, "tp"),
            P("sp", None, "tp"),
            P("sp", "tp", None),
            P("sp", "tp"),
            P("sp", "tp"),
            P("sp", "tp"),
            P("sp", "tp"),
        ),
        check_vma=False,
    )
```

```python
import jax
import jax.numpy as jnp
from jax import lax
from jax.experimental import pallas as pl
from jax.experimental.pallas import tpu as pltpu
from jax.sharding import PartitionSpec as P

MESH = pl.DeviceIdType.MESH
BF = jnp.bfloat16
F32 = jnp.float32
NZ, NX, NY = 8, 4, 4
NSP = NZ * NX
CAP = 16
TOK = 128
CH = 256
D = 2048
FFL = 352
ROWS = NSP * CAP
NK = 8
CR = ROWS // NK
NP = 4
PR = ROWS // NP
ORDER = (0, 1, 7, 3, 5, 4, 2, 6)


def dot(a, b, ca, cb):
    return lax.dot_general(a, b, (((ca,), (cb,)), ((), ())), preferred_element_type=F32)


def kernel(
    out_grad_h,
    moe_input_h,
    weight_h,
    ids_h,
    gate_proj,
    up_proj,
    down_proj,
    out_proj_h,
    conv_out_h,
    gate_b_h,
    gate_c_h,
    value_v_h,
    taps_h,
    g_gate,
    g_up,
    g_down,
    g_out_h,
    g_b_h,
    g_c_h,
    g_v_h,
    out_grad,
    moe_input,
    weight_t,
    ids_t,
    out_proj,
    conv_out,
    gate_b,
    gate_c,
    value_v,
    taps,
    g_out,
    g_b,
    g_c,
    g_v,
    og_gu,
    og_down,
    i_sem,
    o_sem,
    send,
    xd,
    wgu,
    wd,
    place,
    dgu_t,
    hid_t,
    part,
    sib,
    ssum,
    along,
    rsum,
    ret,
    hf,
    js,
    dt,
    mx,
    hsend,
    halo,
    w_sem,
    a_send,
    a_recv,
    b_send,
    b_recv,
    d_send,
    d_recv,
    e_send,
    e_recv,
    h_send,
    h_recv,
    j_send,
    j_recv,
    k_send,
    k_recv,
    m_send,
    m_recv,
    n_send,
    n_recv,
):
    s = lax.axis_index("sp")
    t = lax.axis_index("tp")
    z, x = s // NX, s % NX
    y, c = t // 2, t % 2
    up, down, far = (y + 1) % NY, (y + NY - 1) % NY, (y + 2) % NY
    t_up, t_down, t_sib = up * 2 + c, down * 2 + c, y * 2 + (1 - c)
    t_far = far * 2 + c

    def remote(src, dst, ssem, rsem, sp, tp):
        return pltpu.make_async_remote_copy(
            src_ref=src,
            dst_ref=dst,
            send_sem=ssem,
            recv_sem=rsem,
            device_id={"sp": sp, "tp": tp},
            device_id_type=MESH,
        )

    def arrived(ref, rsem):
        remote(ref, ref, n_send.at[0], rsem, s, t).wait_recv()

    def left(ref, ssem):
        remote(ref, ref, ssem, n_recv.at[0], s, t).wait_send()

    barrier = pltpu.get_barrier_semaphore()

    def greet(i, carry):
        pl.semaphore_signal(
            barrier, inc=1, device_id={"sp": (s + i) % NSP, "tp": t}, device_id_type=MESH
        )
        return carry

    lax.fori_loop(1, NSP, greet, 0)
    for peer in (t_up, t_down, t_far, t_sib):
        pl.semaphore_signal(barrier, inc=1, device_id={"sp": s, "tp": peer}, device_id_type=MESH)
    cross = (z + NZ // 2) % NZ
    back = (t + NZ // 2) % NZ
    for j in range(NX):
        pl.semaphore_signal(
            barrier, inc=1, device_id={"sp": t * NX + j, "tp": cross}, device_id_type=MESH
        )
        pl.semaphore_signal(
            barrier, inc=1, device_id={"sp": back * NX + j, "tp": z}, device_id_type=MESH
        )

    small = [
        pltpu.make_async_copy(a, b, i_sem.at[i])
        for i, (a, b) in enumerate(
            (
                (ids_h, ids_t),
                (weight_h, weight_t),
                (out_grad_h, out_grad),
                (moe_input_h, moe_input),
                (gate_b_h, gate_b),
                (conv_out_h, conv_out),
                (gate_c_h, gate_c),
                (value_v_h, value_v),
                (taps_h, taps),
                (out_proj_h, out_proj),
            )
        )
    ]
    loads = [
        pltpu.make_async_copy(gate_proj.at[0], wgu.at[pl.ds(0, FFL), :], w_sem.at[0]),
        pltpu.make_async_copy(up_proj.at[0], wgu.at[pl.ds(FFL, FFL), :], w_sem.at[1]),
        pltpu.make_async_copy(down_proj.at[0], wd, w_sem.at[2]),
    ]
    for load in small:
        load.start()
    for load in loads:
        load.start()

    for load in small[:6]:
        load.wait()

    ids = ids_t[...]
    experts = lax.broadcasted_iota(jnp.int32, (NSP, TOK), 0)
    e0 = jnp.where(experts == ids[0:1, :], 1.0, 0.0).astype(F32)
    e1 = jnp.where(experts == ids[1:2, :], 1.0, 0.0).astype(F32)
    row = lax.broadcasted_iota(jnp.int32, (TOK, TOK), 0)
    col = lax.broadcasted_iota(jnp.int32, (TOK, TOK), 1)
    earlier = jnp.where(row < col, 1.0, 0.0).astype(BF)
    before = dot((e0 + e1).astype(BF), earlier, 1, 0)
    slot0 = jnp.sum(before * e0, axis=0, keepdims=True)
    slot1 = jnp.sum(before * e1, axis=0, keepdims=True)
    idf = ids.astype(F32) * CAP
    at = lax.broadcasted_iota(jnp.int32, (ROWS, TOK), 0).astype(F32)
    p0 = jnp.where(at == idf[0:1, :] + slot0, 1.0, 0.0).astype(BF)
    p1 = jnp.where(at == idf[1:2, :] + slot1, 1.0, 0.0).astype(BF)
    place[...] = p0 + p1
    og = out_grad[...].astype(F32)
    w = weight_t[...]
    w0 = jnp.broadcast_to(w[0:1, :], (TOK, TOK)).T
    w1 = jnp.broadcast_to(w[1:2, :], (TOK, TOK)).T
    dy0 = (jnp.concatenate([w0, w0], axis=1) * og).astype(BF)
    dy1 = (jnp.concatenate([w1, w1], axis=1) * og).astype(BF)
    send[0] = dot(p0 + p1, moe_input[...], 1, 0).astype(BF)
    send[1] = (dot(p0, dy0, 1, 0) + dot(p1, dy1, 1, 0)).astype(BF)
    mixed = (gate_b[...].astype(F32) * conv_out[...].astype(F32)).astype(BF)
    own_rows = pl.ds(pl.multiple_of((x * NZ + z) * TOK, TOK), TOK)
    mx[own_rows, :] = mixed

    def cols(tp, width=CH):
        return pl.ds(pl.multiple_of(tp * width, width), width)

    pl.semaphore_wait(barrier, NSP - 1 + 4 + 8)

    def a_copy(k, xx):
        target = ((z + ORDER[k]) % NZ) * NX + xx
        src = send.at[:, pl.ds(pl.multiple_of(target * CAP, CAP), CAP), :]
        dst = xd.at[:, pl.ds(pl.multiple_of(k * CR + x * CAP, CAP), CAP), cols(t)]
        return remote(src, dst, a_send.at[k * NX + xx], a_recv.at[k * NX + x], target, t)

    def each_x(first, do):
        def body(i, carry):
            do((x + i) % NX)
            return carry

        lax.fori_loop(first, NX, body, 0)

    def a_start(k):
        each_x(1 if k == 0 else 0, lambda xx: a_copy(k, xx).start())

    def a_wait(k):
        def one(xx):
            arrived(
                xd.at[:, pl.ds(pl.multiple_of(k * CR + xx * CAP, CAP), CAP), cols(t)],
                a_recv.at[k * NX + xx],
            )

        each_x(1 if k == 0 else 0, one)

    here = pl.ds(pl.multiple_of(x * CAP, CAP), CAP)

    def gather(piece, ss, rs):
        def one():
            for i, peer in enumerate((t_sib, t_up, t_down, t_far)):
                remote(piece(t), piece(t), ss(i), rs(i), s, peer).start()

        def two():
            for i, origin in enumerate((t_down, t_up, t_far)):
                arrived(piece(origin), rs(1 + i))
                remote(piece(origin), piece(origin), ss(4 + i), rs(4 + i), s, t_sib).start()

        def three():
            for i, origin in enumerate((y, down, up, far)):
                arrived(piece(origin * 2 + 1 - c), rs(i if i == 0 else 3 + i))

        def end():
            for i in range(7):
                left(piece(t), ss(i))

        return one, two, three, end

    def relay(piece, ss, rs):
        def one():
            for i, peer in enumerate((t_sib, t_up, t_down)):
                remote(piece(t), piece(t), ss(i), rs(i), s, peer).start()

        def two():
            for i, (origin, peer) in enumerate(((t_down, t_up), (t_up, t_down))):
                arrived(piece(origin), rs(1 + i))
                half = piece(origin, i)
                remote(half, half, ss(3 + i), rs(3 + i), s, peer).start()
                remote(piece(origin), piece(origin), ss(5 + i), rs(5 + i), s, t_sib).start()

        def three():
            for i in range(2):
                half = piece(t_far, i)
                arrived(half, rs(3 + i))
                remote(half, half, ss(7 + i), rs(7 + i), s, t_sib).start()

        def four():
            arrived(piece(t_sib), rs(0))
            arrived(piece(down * 2 + 1 - c), rs(5))
            arrived(piece(up * 2 + 1 - c), rs(6))
            arrived(piece(far * 2 + 1 - c, 0), rs(7))
            arrived(piece(far * 2 + 1 - c, 1), rs(8))

        def end():
            for i in range(9):
                left(piece(t) if i in (0, 1, 2, 5, 6) else piece(t, 0), ss(i))

        return one, two, three, four, end

    def chunk_piece(k):
        rows = pl.ds(k * CR, CR)

        def piece(tp, half=None):
            if half is None:
                return xd.at[:, rows, cols(tp)]
            return xd.at[half, rows, cols(tp)]

        return piece

    chunk = [
        relay(
            chunk_piece(k),
            lambda i, k=k: b_send.at[k * 9 + i],
            lambda i, k=k: b_recv.at[k * 9 + i],
        )
        for k in range(NK)
    ]

    def block(zz, xx, half=None):
        base = (xx * NZ + zz) * TOK
        if half is None:
            return mx.at[pl.ds(pl.multiple_of(base, TOK), TOK), :]
        return mx.at[pl.ds(pl.multiple_of(base + half * (TOK // 2), TOK // 2), TOK // 2), :]

    z_up, z_down = ((z + 1) % NZ) * NX + x, ((z + NZ - 1) % NZ) * NX + x
    x_up, x_down, x_far = (x + 1) % NX, (x + NX - 1) % NX, (x + 2) % NX

    def z_hop(r):
        low, high = (0, 1) if r == 4 else (None, None)
        a = block((z + NZ - (r - 1)) % NZ, x, low)
        b = block((z + r - 1) % NZ, x, high)
        remote(a, a, n_send.at[2 * r], n_recv.at[2 * r], z_up, t).start()
        remote(b, b, n_send.at[2 * r + 1], n_recv.at[2 * r + 1], z_down, t).start()

    def z_arrived(r):
        low, high = (0, 1) if r == 4 else (None, None)
        arrived(block((z + NZ - r) % NZ, x, low), n_recv.at[2 * r])
        arrived(block((z + r) % NZ, x, high), n_recv.at[2 * r + 1])

    def x_hop(d):
        a = block((z + d) % NZ, x)
        for i, to in enumerate((x_up, x_down, x_far)):
            remote(a, a, m_send.at[3 * d + i], m_recv.at[3 * d + i], z * NX + to, t).start()

    def forward(lo, hi):
        rows = pl.ds(lo * CR, (hi - lo) * CR)
        gu = dot(wgu[...], xd[0, rows, :], 1, 1)
        dh = dot(wd[...], xd[1, rows, :], 1, 1)
        g, u = gu[:FFL], gu[FFL:]
        sig = 1.0 / (1.0 + jnp.exp(-g))
        act = g * sig
        hid_t[:, rows] = (act * u).astype(BF)
        dgu_t[0:FFL, rows] = (dh * u * (sig * (1.0 + g * (1.0 - sig)))).astype(BF)
        dgu_t[FFL : 2 * FFL, rows] = (dh * act).astype(BF)

    def grads(lo, hi):
        def body(i, carry):
            cs = cols(i)
            og_gu[:, cs] = dot(dgu_t[...], xd[0, :, cs], 1, 0).astype(BF)
            og_down[:, cs] = dot(hid_t[...], xd[1, :, cs], 1, 0).astype(BF)
            return carry

        lax.fori_loop(lo, hi, body, 0)

    def dx(m):
        rows = pl.ds(m * PR, PR)
        dg = dgu_t[:, rows].T

        def body(i, carry):
            part[i % 2, i // 2, rows, :] = dot(dg, wgu[:, cols(i)], 1, 0).astype(BF)
            return carry

        lax.fori_loop(0, 8, body, 0)

    def d_rows(m):
        return pl.ds(m * PR, PR)

    def d0(m):
        remote(
            part.at[1 - c, :, d_rows(m), :],
            sib.at[:, d_rows(m), :],
            d_send.at[m * 4],
            d_recv.at[m * 4],
            s,
            t_sib,
        ).start()

    def d1(m):
        arrived(sib.at[:, d_rows(m), :], d_recv.at[m * 4])
        ssum[:, d_rows(m), :] = (
            part[c, :, d_rows(m), :].astype(F32) + sib[:, d_rows(m), :].astype(F32)
        ).astype(BF)
        for i, (to, peer) in enumerate(((far, t_far), (up, t_up), (down, t_down))):
            remote(
                ssum.at[to, d_rows(m), :],
                along.at[i, d_rows(m), :],
                d_send.at[m * 4 + 1 + i],
                d_recv.at[m * 4 + 1 + i],
                s,
                peer,
            ).start()

    def e_copy(k, xx):
        target = ((z + NZ - ORDER[k]) % NZ) * NX + xx
        i = k * NX + xx
        return remote(
            rsum.at[pl.ds(pl.multiple_of(i * CAP, CAP), CAP), :],
            ret.at[pl.ds(pl.multiple_of(s * CAP, CAP), CAP), :],
            e_send.at[i],
            e_recv.at[s],
            target,
            t,
        )

    def d3(m):
        for i in range(3):
            arrived(along.at[i, d_rows(m), :], d_recv.at[m * 4 + 1 + i])
        rsum[d_rows(m), :] = (
            ssum[y, d_rows(m), :].astype(F32)
            + along[0, d_rows(m), :].astype(F32)
            + along[1, d_rows(m), :].astype(F32)
            + along[2, d_rows(m), :].astype(F32)
        ).astype(BF)
        for k in (2 * m, 2 * m + 1):
            each_x(1 if k == 0 else 0, lambda xx: e_copy(k, xx).start())
        if m == 0:
            ret[pl.ds(pl.multiple_of(s * CAP, CAP), CAP), :] = rsum[here, :]

    z_hop(1)
    for k in range(NK):
        a_start(k)
    xd[:, here, cols(t)] = send[:, pl.ds(pl.multiple_of(s * CAP, CAP), CAP), :]
    x_hop(0)
    for k in range(NK):
        a_wait(k)
        chunk[k][0]()
        if k >= 2:
            chunk[k - 2][1]()
        if k >= 4:
            chunk[k - 4][2]()
        if k == 4:
            z_arrived(1)
            z_hop(2)
            x_hop(1)
            x_hop(7)
        if k == 6:
            z_arrived(2)
            z_hop(3)
            x_hop(2)
            x_hop(6)
    chunk[6][1]()
    chunk[4][2]()
    for load in loads:
        load.wait()
    chunk[0][3]()
    chunk[1][3]()
    chunk[2][3]()
    chunk[3][3]()
    forward(0, 4)
    chunk[7][1]()
    chunk[5][2]()
    dx(0)
    d0(0)
    chunk[6][2]()
    dx(1)
    d0(1)
    d1(0)
    z_arrived(3)
    z_hop(4)
    x_hop(3)
    x_hop(5)
    chunk[7][2]()
    chunk[4][3]()
    chunk[5][3]()
    forward(4, 6)
    d1(1)
    dx(2)
    d0(2)
    chunk[6][3]()
    chunk[7][3]()
    forward(6, 8)
    d1(2)
    dx(3)
    d0(3)
    d3(0)
    z_arrived(4)
    x_hop(4)
    d3(1)
    d1(3)
    grads(0, 2)
    d3(2)
    d3(3)
    grads(2, 8)
    stores = [
        pltpu.make_async_copy(og_gu.at[pl.ds(0, FFL), :], g_gate.at[0], o_sem.at[0]),
        pltpu.make_async_copy(og_gu.at[pl.ds(FFL, FFL), :], g_up.at[0], o_sem.at[1]),
        pltpu.make_async_copy(og_down, g_down.at[0], o_sem.at[2]),
    ]
    for store in stores:
        store.start()
    for load in small[6:]:
        load.wait()

    def e_wait(i, carry):
        e = (s + i) % NSP
        arrived(ret.at[pl.ds(pl.multiple_of(e * CAP, CAP), CAP), :], e_recv.at[e])
        return carry

    lax.fori_loop(1, NSP, e_wait, 0)

    dh = out_grad[...].astype(F32) + dot(place[...], ret[...], 0, 0)
    js[...] = dh.T.astype(BF)
    hf[:, cols(t)] = dh.astype(BF)

    def token_cols(zz, xx):
        return pl.ds(pl.multiple_of((xx * NZ + zz) * TOK, TOK), TOK)

    for j in range(NX):
        remote(
            js.at[pl.ds(64 * j, 64), :],
            dt.at[:, token_cols(z, x)],
            j_send.at[j],
            j_recv.at[x],
            t * NX + j,
            cross,
        ).start()

    def h_piece(tp):
        return hf.at[:, cols(tp)]

    x_order = (x, (x + 1) % NX, (x + NX - 1) % NX, (x + 2) % NX)

    def j_piece(i):
        return lambda tp: dt.at[:, token_cols((tp + NZ // 2) % NZ, x_order[i])]

    hg = gather(h_piece, lambda i: h_send.at[i], lambda i: h_recv.at[i])
    jg = [
        gather(
            j_piece(i),
            lambda n, i=i: k_send.at[7 * i + n],
            lambda n, i=i: k_recv.at[7 * i + n],
        )
        for i in range(NX)
    ]
    hg[0]()
    for k in range(NK):
        each_x(1 if k == 0 else 0, lambda xx: a_copy(k, xx).wait_send())
        each_x(1 if k == 0 else 0, lambda xx: e_copy(k, xx).wait_send())
        chunk[k][4]()
    for m in range(NP):
        left(part.at[0, :, d_rows(m), :], d_send.at[m * 4])
        for i in range(3):
            left(along.at[i, d_rows(m), :], d_send.at[m * 4 + 1 + i])
    for d in range(NZ):
        for i in range(3):
            left(block(z, x), m_send.at[3 * d + i])
    for r in range(1, 5):
        half = 0 if r == 4 else None
        left(block(z, x, half), n_send.at[2 * r])
        left(block(z, x, half), n_send.at[2 * r + 1])
    hg[1]()
    for i in range(NX):
        arrived(dt.at[:, token_cols(back, x_order[i])], j_recv.at[x_order[i]])
        jg[i][0]()
    hg[2]()
    dz = dot(hf[...], out_proj[...], 1, 0)
    dconv = (dz * gate_b[...].astype(F32)).astype(BF)
    hsend[...] = dconv

    @pl.when(s < NSP - 1)
    def _():
        remote(
            hsend.at[pl.ds(TOK - 16, 16), :], halo.at[0], j_send.at[4], j_recv.at[4], s + 1, t
        ).start()

    @pl.when(s > 0)
    def _():
        remote(hsend.at[pl.ds(0, 16), :], halo.at[1], j_send.at[5], j_recv.at[5], s - 1, t).start()

    for i in range(NX):
        jg[i][1]()
    g_b[...] = (dz * conv_out[...].astype(F32)).astype(BF)

    @pl.when(s > 0)
    def _():
        arrived(halo.at[0], j_recv.at[4])

    @pl.when(s == 0)
    def _():
        halo[0] = jnp.zeros((16, CH), BF)

    @pl.when(s < NSP - 1)
    def _():
        arrived(halo.at[1], j_recv.at[5])

    @pl.when(s == NSP - 1)
    def _():
        halo[1] = jnp.zeros((16, CH), BF)

    d = dconv.astype(F32)
    at_row = lax.broadcasted_iota(jnp.int32, (TOK, CH), 0)
    before_first = halo[0].astype(F32)[15:16, :]
    after_last = halo[1].astype(F32)[0:1, :]
    earlier_rows = jnp.where(at_row == 0, before_first, pltpu.roll(d, 1, 0))
    later_rows = jnp.where(at_row == TOK - 1, after_last, pltpu.roll(d, TOK - 1, 0))
    tp3 = taps[...]
    grad_u = tp3[0:1, :] * later_rows + tp3[1:2, :] * d + tp3[2:3, :] * earlier_rows
    g_c[...] = (grad_u * value_v[...].astype(F32)).astype(BF)
    g_v[...] = (grad_u * gate_c[...].astype(F32)).astype(BF)

    for d in range(NZ):
        for i, source in enumerate((x_down, x_up, x_far)):
            arrived(block((z + d) % NZ, source), m_recv.at[3 * d + i])
    total = jnp.zeros((64, CH), F32)
    for i in range(NX):
        jg[i][2]()
        ks = pl.ds(pl.multiple_of(x_order[i] * (NZ * TOK), NZ * TOK), NZ * TOK)
        total += dot(dt[:, ks], mx[ks, :], 1, 0)
    g_out[...] = total
    late = [
        pltpu.make_async_copy(a, b, o_sem.at[3 + i])
        for i, (a, b) in enumerate(((g_out, g_out_h), (g_b, g_b_h), (g_c, g_c_h), (g_v, g_v_h)))
    ]
    for store in late:
        store.start()
    stores += late

    hg[3]()
    for i in range(NX):
        jg[i][3]()
    for j in range(NX):
        left(js.at[pl.ds(64 * j, 64), :], j_send.at[j])

    @pl.when(s < NSP - 1)
    def _():
        left(halo.at[0], j_send.at[4])

    @pl.when(s > 0)
    def _():
        left(halo.at[1], j_send.at[5])

    for store in stores:
        store.wait()


def emit(*refs):
    ins, outs, held = refs[:7], refs[7:14], refs[14:21]
    i_sem, o_sem = refs[21:]
    pieces = []
    for a, b, v in zip(ins, outs, held):
        if len(a.shape) == 3:
            half = a.shape[1] // 2
            pieces += [tuple(r.at[:, pl.ds(i * half, half), :] for r in (a, b, v)) for i in range(2)]
        else:
            pieces.append((a, b, v))
    loads = [pltpu.make_async_copy(a, v, i_sem.at[i]) for i, (a, _, v) in enumerate(pieces)]
    stores = [pltpu.make_async_copy(v, b, o_sem.at[i]) for i, (_, b, v) in enumerate(pieces)]
    for load in loads:
        load.start()
    for load, store in zip(loads, stores):
        load.wait()
        store.start()
    for store in stores:
        store.wait()


def local(
    out_grad,
    moe_input,
    route_weight,
    route_ids,
    gate_proj,
    up_proj,
    down_proj,
    out_proj,
    conv_out,
    gate_b,
    gate_c,
    value_v,
    conv_taps,
):
    hbm = pl.BlockSpec(memory_space=pl.ANY)
    dma = pltpu.SemaphoreType.DMA
    shape = jax.ShapeDtypeStruct
    kept = pl.pallas_call(
        kernel,
        out_shape=(
            shape((1, FFL, D), BF),
            shape((1, FFL, D), BF),
            shape((1, FFL, D), BF),
            shape((64, CH), F32),
            shape((TOK, CH), BF),
            shape((TOK, CH), BF),
            shape((TOK, CH), BF),
        ),
        in_specs=[hbm] * 13,
        out_specs=(hbm,) * 7,
        scratch_shapes=[
            pltpu.VMEM((TOK, CH), BF),
            pltpu.VMEM((TOK, CH), BF),
            pltpu.VMEM((2, TOK), F32),
            pltpu.VMEM((2, TOK), jnp.int32),
            pltpu.VMEM((D, CH), BF),
            pltpu.VMEM((TOK, CH), BF),
            pltpu.VMEM((TOK, CH), BF),
            pltpu.VMEM((TOK, CH), BF),
            pltpu.VMEM((TOK, CH), BF),
            pltpu.VMEM((3, CH), F32),
            pltpu.VMEM((64, CH), F32),
            pltpu.VMEM((TOK, CH), BF),
            pltpu.VMEM((TOK, CH), BF),
            pltpu.VMEM((TOK, CH), BF),
            pltpu.VMEM((2 * FFL, D), BF),
            pltpu.VMEM((FFL, D), BF),
            dma((10,)),
            dma((7,)),
            pltpu.VMEM((2, ROWS, CH), BF),
            pltpu.VMEM((2, ROWS, D), BF),
            pltpu.VMEM((2 * FFL, D), BF),
            pltpu.VMEM((FFL, D), BF),
            pltpu.VMEM((ROWS, TOK), BF),
            pltpu.VMEM((2 * FFL, ROWS), BF),
            pltpu.VMEM((FFL, ROWS), BF),
            pltpu.VMEM((2, NY, ROWS, CH), BF),
            pltpu.VMEM((NY, ROWS, CH), BF),
            pltpu.VMEM((NY, ROWS, CH), BF),
            pltpu.VMEM((3, ROWS, CH), BF),
            pltpu.VMEM((ROWS, CH), BF),
            pltpu.VMEM((ROWS, CH), BF),
            pltpu.VMEM((TOK, D), BF),
            pltpu.VMEM((CH, TOK), BF),
            pltpu.VMEM((64, NSP * TOK), BF),
            pltpu.VMEM((NSP * TOK, CH), BF),
            pltpu.VMEM((TOK, CH), BF),
            pltpu.VMEM((2, 16, CH), BF),
            dma((3,)),
            dma((NSP,)),
            dma((NSP,)),
            dma((9 * NK,)),
            dma((9 * NK,)),
            dma((4 * NP,)),
            dma((4 * NP,)),
            dma((NSP,)),
            dma((NSP,)),
            dma((7,)),
            dma((7,)),
            dma((6,)),
            dma((6,)),
            dma((7 * NX,)),
            dma((7 * NX,)),
            dma((3 * NZ,)),
            dma((3 * NZ,)),
            dma((10,)),
            dma((10,)),
        ],
        compiler_params=pltpu.CompilerParams(
            collective_id=0, has_side_effects=True, vmem_limit_bytes=60 * 1024 * 1024
        ),
        name="layer",
    )(
        out_grad,
        moe_input,
        route_weight.T,
        route_ids.T,
        gate_proj.transpose(0, 2, 1),
        up_proj.transpose(0, 2, 1),
        down_proj,
        out_proj,
        conv_out,
        gate_b,
        gate_c,
        value_v,
        conv_taps,
    )
    g_gate, g_up, g_down, g_out, g_b, g_c, g_v = pl.pallas_call(
        emit,
        out_shape=tuple(shape(a.shape, a.dtype) for a in kept),
        in_specs=[hbm] * 7,
        out_specs=(hbm,) * 7,
        scratch_shapes=[pltpu.VMEM(a.shape, a.dtype) for a in kept] + [dma((10,)), dma((10,))],
        compiler_params=pltpu.CompilerParams(vmem_limit_bytes=60 * 1024 * 1024),
        name="emit",
    )(*kept)
    return g_gate.transpose(0, 2, 1), g_up.transpose(0, 2, 1), g_down, g_out, g_b, g_c, g_v


def solution(mesh):
    return jax.shard_map(
        local,
        mesh=mesh,
        in_specs=(
            P("sp", "tp"),
            P("sp", "tp"),
            P("sp", None),
            P("sp", None),
            P("sp", None, "tp"),
            P("sp", None, "tp"),
            P("sp", "tp", None),
            P(None, "tp"),
            P("sp", "tp"),
            P("sp", "tp"),
            P("sp", "tp"),
            P("sp", "tp"),
            P(None, "tp"),
        ),
        out_specs=(
            P("sp", None, "tp"),
            P("sp", None, "tp"),
            P("sp", "tp", None),
            P("sp", "tp"),
            P("sp", "tp"),
            P("sp", "tp"),
            P("sp", "tp"),
        ),
        check_vma=False,
    )
```
